32 devices in a mesh: sp: 4 (over z), fs: 4 (over y, x), tp: 2 (over core).
Axes of the slice: x: 2, y: 2, z: 4, core: 2. Of those that a mesh axis runs over, the one named last changes fastest.
Arguments:
- tokens: bfloat16 [4, 1024, 2048], P('fs', 'sp', 'tp'), may hold values from -6 to 6
- norm_gain: float32 [2048], replicated, may hold values from 0.1 to 1.9
- query_weight: bfloat16 [2048, 1024], P('fs', 'tp'), may hold values from -1 to 1
- key_weight: bfloat16 [2048, 1024], P('fs', 'tp'), may hold values from -4 to 4
- value_weight: bfloat16 [2048, 1024], P('fs', 'tp'), may hold values from -0.125 to 0.125
- state_query: bfloat16 [2048, 1024], P('fs', 'tp'), may hold values from -0.125 to 0.125
- state_key: bfloat16 [2048, 1024], P('fs', 'tp'), may hold values from -0.125 to 0.125
- state_value: bfloat16 [2048, 1024], P('fs', 'tp'), may hold values from -0.125 to 0.125
- map_lambda: float32 [8], P('tp'), may hold values from 0.3 to 0.8
- diff_gain: float32 [1024], P('tp'), may hold values from 0.1 to 1.9
- decay_rate: float32 [8], P('tp'), may hold values from 0 to 0.04
- state_gain: float32 [1024], P('tp'), may hold values from 0.1 to 1.9
- out_weight: bfloat16 [2048, 2048], replicated, may hold values from -0.125 to 0.125
Outputs:
- mixed: bfloat16 [4, 1024, 2048], P('fs', ('sp', 'tp'))
The draws below stay inside these ranges and needn't reach their ends.
All inputs are finite; a program needn't handle non-finite values.
Results may differ from the reference program's by a relative error of at most 0.015.
Values may be sent and summed in bfloat16 or wider, within the bound.
A program may use at most 128 MiB of HBM per device.

```python
import math
import jax
import jax.numpy as jnp
from jax import lax

D = 2048
HD = 8
DK = 64
DV = 128
HR = 8
DR = 128
TOK_DEV = 256
LENGTH = 1024
SEQS = 4


def query_base(key):
    return jax.random.normal(jax.random.fold_in(key, 101), (D, HD * 2 * DK), jnp.float32) * (2.0 / D) ** 0.5


def draw_query_weight(key, part):
    return jnp.clip(query_base(key), -1.0, 1.0).astype(jnp.bfloat16)


def draw_key_weight(key, part):
    fresh = jax.random.normal(jax.random.fold_in(key, 202), (D, HD * 2 * DK), jnp.float32) * (2.0 / D) ** 0.5
    result = fresh
    return jnp.clip(result, -4.0, 4.0).astype(jnp.bfloat16)


def draw_decay_rate(key, part):
    pick = jax.random.uniform(jax.random.fold_in(key, 404), (HR,), jnp.float32)
    share = 0.5
    slow_rate = jnp.exp(jax.random.uniform(jax.random.fold_in(key, 505), (HR,), jnp.float32, math.log(0.1), math.log(2.0))) / LENGTH
    fast_rate = jnp.exp(jax.random.uniform(jax.random.fold_in(key, 606), (HR,), jnp.float32, math.log(0.01), math.log(0.033)))
    return jnp.where(pick < share, slow_rate, fast_rate)


def shard_levels(key, shape, pieces, smallest, high):
    level, own = 1.0, jax.random.fold_in(key, 6)
    for dim, blocks in pieces:
        steps = jnp.exp(jax.random.uniform(jax.random.fold_in(own, dim), (blocks,), jnp.float32, smallest / len(pieces), high / len(pieces)))
        level = level * jnp.repeat(steps, shape[dim] // blocks).reshape([-1 if axis == dim else 1 for axis in range(len(shape))])
    return level


def scatter_about(rng, dims, width, most, shards=(), held_as=jnp.bfloat16):
    drawn = width * jax.random.normal(rng, dims, jnp.float32)
    if shards:
        drawn = drawn * shard_levels(rng, dims, shards, -0.22, 0.18)
    return jnp.clip(drawn, -most, most).astype(held_as)


def setup_inputs(seed: int = 0) -> dict:
    key_list = jax.random.split(jax.random.key(seed), 14)
    return {
        "tokens": scatter_about(key_list[0], (SEQS, LENGTH, D), 1.0, 6.0, ((0, 4), (1, 4), (2, 2))),
        "norm_gain": jnp.clip(1.0 + 0.18 * jax.random.normal(key_list[1], (D,), jnp.float32), 0.1, 1.9),
        "query_weight": draw_query_weight(jax.random.fold_in(key_list[13], 71), 0),
        "key_weight": draw_key_weight(jax.random.fold_in(key_list[13], 71), 0),
        "value_weight": scatter_about(key_list[4], (D, HD * DV), D ** -0.5, 0.125, ((0, 4), (1, 2))),
        "state_query": scatter_about(key_list[5], (D, HR * DR), D ** -0.5, 0.125, ((0, 4), (1, 2))),
        "state_key": scatter_about(key_list[6], (D, HR * DR), D ** -0.5, 0.125, ((0, 4), (1, 2))),
        "state_value": scatter_about(key_list[7], (D, HR * DR), D ** -0.5, 0.125, ((0, 4), (1, 2))),
        "map_lambda": jnp.clip(0.3 + 0.5 * jax.random.uniform(key_list[8], (HD,), jnp.float32) ** shard_levels(key_list[8], (HD,), ((0, 2),), -0.2, 0.2), 0.3, 0.8),
        "diff_gain": jnp.clip(1.0 + 0.18 * jax.random.normal(key_list[9], (HD * DV,), jnp.float32), 0.1, 1.9),
        "decay_rate": draw_decay_rate(jax.random.fold_in(key_list[13], 71), 0),
        "state_gain": jnp.clip(1.0 + 0.18 * jax.random.normal(key_list[11], (HR * DR,), jnp.float32), 0.1, 1.9),
        "out_weight": scatter_about(key_list[12], (HD * DV + HR * DR, D), (HD * DV + HR * DR) ** -0.5, 0.125),
    }


epsilon = 1e-05
branch_scale = 0.8
masked_score = -1e+30

def normalize(values, gain):
    meansq = lax.optimization_barrier(jnp.mean(values * values, axis=-1, keepdims=True))
    return values * lax.rsqrt(meansq + epsilon) * gain

def rounded(values):
    return lax.optimization_barrier(values.astype(jnp.bfloat16)).astype(jnp.float32)

def differential(att_query, att_keys, att_values, map_lambda, diff_gain):
    length = att_query.shape[0]
    blocks = length // TOK_DEV
    query_float = att_query.reshape(blocks, TOK_DEV, HD, 2, DK).astype(jnp.float32)
    key_float = att_keys.reshape(length, HD, 2, DK).astype(jnp.float32)
    value_float = att_values.reshape(length, HD, DV).astype(jnp.float32)
    key_place = jnp.arange(length)

    def one_block(inputs):
        block_index, query_block = inputs
        query_place = block_index * TOK_DEV + jnp.arange(TOK_DEV)
        scores = jnp.einsum('qhmd,khmd->mhqk', query_block, key_float) * DK ** (-0.5)
        causal = key_place[None, :] <= query_place[:, None]
        row_peak = lax.optimization_barrier(jnp.max(jnp.where(causal, scores, masked_score), axis=-1, keepdims=True))
        weights = jnp.where(causal, jnp.exp(scores - row_peak), 0.0)
        totals = lax.optimization_barrier(jnp.sum(weights, axis=-1, keepdims=True))
        averaged = jnp.einsum('mhqk,khv->mhqv', rounded(weights), value_float) / totals
        differ = averaged[0] - map_lambda[:, None, None] * averaged[1]
        normed = normalize(differ, diff_gain.reshape(HD, 1, DV)) * branch_scale
        return normed.transpose(1, 0, 2).reshape(TOK_DEV, HD * DV).astype(jnp.bfloat16)
    outputs = lax.map(one_block, (jnp.arange(blocks), query_float))
    return outputs.reshape(length, HD * DV)

def retention(ret_query, ret_keys, ret_values, decay_rate, state_gain):
    length = ret_query.shape[0]
    blocks = length // TOK_DEV

    def to_blocks(array):
        return array.reshape(blocks, TOK_DEV, HR, DR)
    position = jnp.arange(TOK_DEV).astype(jnp.float32)
    distance = position[:, None] - position[None, :]
    decay_col = decay_rate[:, None, None]
    within = jnp.where(distance >= 0, jnp.exp(-decay_col * jnp.maximum(distance, 0.0)), 0.0)
    query_decay = jnp.exp(-decay_col * (position + 1.0)[None, :, None])
    key_decay = jnp.exp(-decay_rate[None, :, None] * (TOK_DEV - 1.0 - position)[:, None, None])
    block_decay = jnp.exp(-decay_rate * TOK_DEV)[:, None, None]

    def advance(carry_state, inputs):
        query_block, key_block, value_block = (member.astype(jnp.float32) for member in inputs)
        local_scores = jnp.einsum('qhd,khd->hqk', query_block, key_block) * within
        intra_out = jnp.einsum('hqk,khv->hqv', rounded(local_scores), value_block)
        carried = jnp.einsum('qhd,hdv->hqv', query_block, carry_state, precision=lax.Precision.HIGHEST) * query_decay
        carry_state = carry_state * block_decay + jnp.einsum('khd,khv->hdv', key_block * key_decay, value_block, precision=lax.Precision.HIGHEST)
        normed = normalize(intra_out + carried, state_gain.reshape(HR, 1, DR))
        return (carry_state, normed.transpose(1, 0, 2).reshape(TOK_DEV, HR * DR).astype(jnp.bfloat16))
    initial = jnp.zeros((HR, DR, DR), jnp.float32)
    _, outputs = lax.scan(advance, initial, (to_blocks(ret_query), to_blocks(ret_keys), to_blocks(ret_values)))
    return outputs.reshape(length, HR * DR)

def reference(tokens, norm_gain, query_weight, key_weight, value_weight, state_query, state_key, state_value, map_lambda, diff_gain, decay_rate, state_gain, out_weight):

    def one_sequence(sequence):
        tok_float = sequence.astype(jnp.float32)
        normed = normalize(tok_float, norm_gain).astype(jnp.bfloat16)

        def project(weight):
            return jnp.dot(normed, weight, preferred_element_type=jnp.float32).astype(jnp.bfloat16)
        attended = differential(project(query_weight), project(key_weight), project(value_weight), map_lambda, diff_gain)
        retained = retention(project(state_query), project(state_key), project(state_value), decay_rate, state_gain)
        joined = jnp.concatenate([attended, retained], axis=1)
        return jnp.dot(joined, out_weight, preferred_element_type=jnp.float32).astype(jnp.bfloat16)
    return lax.map(one_sequence, tokens)
```

```python
import functools

import jax
import jax.numpy as jnp
from jax import lax
from jax.experimental import pallas as pl
from jax.experimental.pallas import tpu as pltpu
from jax.sharding import PartitionSpec as P

DK = 64
DV = 128
DR = 128


epsilon = 1e-05
branch_scale = 0.8
masked_score = -1e30


def from_behind(x, axis, by):
    size = lax.axis_size(axis)
    pairs = [(i, i + by) for i in range(size) if 0 <= i + by < size]
    return lax.ppermute(x, axis, pairs)


def entering(x, axis, join, neutral):
    place = lax.axis_index(axis)
    gathered = jax.tree.map(
        lambda a, kind: lax.all_gather(a.astype(kind), axis), x, (jnp.bfloat16, jnp.bfloat16)
    )
    state = jax.tree.map(lambda a, e: jnp.zeros_like(a) + jnp.asarray(e, a.dtype), x, neutral)

    def one(turn, state):
        return join(
            state,
            jax.tree.map(
                lambda a, own: lax.dynamic_index_in_dim(a, turn, 0, False).astype(own.dtype),
                gathered,
                x,
            ),
        )

    return lax.fori_loop(0, place, one, state)


def attend(att_query, att_keys, att_values, map_lambda, diff_gain):
    tok_rows = att_query.shape[0]
    head_count = map_lambda.shape[0]
    key_width = att_keys.shape[1]
    query_heads = att_query.reshape(tok_rows, head_count, 2, DK)
    sp_index = lax.axis_index("sp")
    query_place = sp_index * tok_rows + jnp.arange(tok_rows)
    score_scale = DK ** (-0.5)

    def absorb_block(running, inputs):
        key_block, key_place = inputs
        key_heads = key_block[:, :key_width].reshape(tok_rows, head_count, 2, DK)
        value_heads = key_block[:, key_width:].reshape(tok_rows, head_count, DV)
        scores = (
            jnp.einsum(
                "qhmd,khmd->mhqk", query_heads, key_heads, preferred_element_type=jnp.float32
            )
            * score_scale
        )
        causal = key_place[None, :] <= query_place[:, None]
        row_peak, totals, summed = running
        new_peak = jnp.maximum(row_peak, jnp.max(jnp.where(causal, scores, masked_score), axis=-1))
        weights = jnp.where(causal, jnp.exp(scores - new_peak[..., None]), 0.0)
        factor = jnp.exp(row_peak - new_peak)
        totals = totals * factor + jnp.sum(weights, axis=-1)
        summed = summed * factor[..., None] + jnp.einsum(
            "mhqk,khv->mhqv",
            weights.astype(jnp.bfloat16),
            value_heads,
            preferred_element_type=jnp.float32,
        )
        return ((new_peak, totals, summed), None)

    def absorb(running, pieces, first_row):
        piece_rows = pieces.shape[0]
        stacked = pieces.reshape(piece_rows // tok_rows, tok_rows, pieces.shape[1])
        places = (first_row + jnp.arange(piece_rows)).reshape(piece_rows // tok_rows, tok_rows)
        return lax.scan(absorb_block, running, (stacked, places))[0]

    starting = (
        jnp.full((2, head_count, tok_rows), masked_score, jnp.float32),
        jnp.zeros((2, head_count, tok_rows), jnp.float32),
        jnp.zeros((2, head_count, tok_rows, DV), jnp.float32),
    )
    joined_kv = jnp.concatenate([att_keys, att_values], axis=1)
    first_state = absorb(starting, joined_kv, sp_index * tok_rows)

    def relay_step(step_index, relay_state):
        running, moving = relay_state
        moving = from_behind(moving, "sp", 1)
        first_row = (sp_index - step_index) * tok_rows
        running = lax.cond(
            first_row >= 0,
            lambda holding: absorb(holding, moving, first_row),
            lambda holding: holding,
            running,
        )
        return (running, moving)

    running, _ = lax.fori_loop(1, lax.axis_size("sp"), relay_step, (first_state, joined_kv))
    row_peak, totals, summed = running
    averaged = summed / totals[..., None]
    differ = averaged[0] - map_lambda[:, None, None] * averaged[1]
    normed = differ * lax.rsqrt(jnp.mean(differ * differ, axis=-1, keepdims=True) + epsilon)
    normed = normed * diff_gain.reshape(head_count, 1, DV) * branch_scale
    return normed.transpose(1, 0, 2).reshape(tok_rows, head_count * DV).astype(jnp.bfloat16)


def retain(ret_query, ret_keys, ret_values, decay_rate, state_gain):
    tok_rows = ret_query.shape[0]
    head_count = decay_rate.shape[0]
    query_heads = ret_query.reshape(tok_rows, head_count, DR)
    key_heads = ret_keys.reshape(tok_rows, head_count, DR)
    value_heads = ret_values.reshape(tok_rows, head_count, DR)
    position = jnp.arange(tok_rows).astype(jnp.float32)
    distance = position[:, None] - position[None, :]
    decay_col = decay_rate[:, None, None]
    within = jnp.where(distance >= 0, jnp.exp(-decay_col * jnp.maximum(distance, 0.0)), 0.0)
    local_scores = (
        jnp.einsum("qhd,khd->hqk", query_heads, key_heads, preferred_element_type=jnp.float32)
        * within
    )
    intra_out = jnp.einsum(
        "hqk,khv->hqv",
        local_scores.astype(jnp.bfloat16),
        value_heads,
        preferred_element_type=jnp.float32,
    )
    key_decayed = key_heads.astype(jnp.float32) * jnp.exp(
        -decay_rate[None, :, None] * (tok_rows - 1.0 - position)[:, None, None]
    )
    own_state = jnp.einsum(
        "khd,khv->hdv",
        key_decayed,
        value_heads.astype(jnp.float32),
        precision=lax.Precision.HIGHEST,
    )
    block_decay = jnp.exp(-decay_rate * tok_rows)

    def link_states(earlier, later):
        return (earlier[0] * later[1][:, None, None] + later[0], earlier[1] * later[1])

    identity = (jnp.zeros_like(own_state), jnp.ones_like(block_decay))
    incoming, _ = entering((own_state, block_decay), "sp", link_states, identity)
    carried = jnp.einsum(
        "qhd,hdv->hqv", query_heads.astype(jnp.float32), incoming, precision=lax.Precision.HIGHEST
    )
    carried = carried * jnp.exp(-decay_col * (position + 1.0)[None, :, None])
    combined = intra_out + carried
    normed = combined * lax.rsqrt(jnp.mean(combined * combined, axis=-1, keepdims=True) + epsilon)
    normed = normed * state_gain.reshape(head_count, 1, DR)
    return normed.transpose(1, 0, 2).reshape(tok_rows, head_count * DR).astype(jnp.bfloat16)


def spread_body(
    tokens,
    norm_gain,
    query_weight,
    key_weight,
    value_weight,
    state_query,
    state_key,
    state_value,
    map_lambda,
    diff_gain,
    decay_rate,
    state_gain,
    out_weight,
):
    gathered = lax.all_gather(tokens[0], "tp", axis=1, tiled=True)
    tok_float = gathered.astype(jnp.float32)
    normed = tok_float * lax.rsqrt(
        jnp.mean(tok_float * tok_float, axis=-1, keepdims=True) + epsilon
    )
    normed = (normed * norm_gain).astype(jnp.bfloat16)
    pieces = (
        lax.all_gather(query_weight, "fs", axis=0, tiled=True),
        lax.all_gather(key_weight, "fs", axis=0, tiled=True),
        lax.all_gather(value_weight, "fs", axis=0, tiled=True),
        lax.all_gather(state_query, "fs", axis=0, tiled=True),
        lax.all_gather(state_key, "fs", axis=0, tiled=True),
        lax.all_gather(state_value, "fs", axis=0, tiled=True),
    )
    projected = tuple(
        (jnp.dot(normed, row_block, preferred_element_type=jnp.float32) for row_block in pieces)
    )
    att_query, att_keys, att_values, ret_query, ret_keys, ret_values = (
        member.astype(jnp.bfloat16) for member in projected
    )
    attended = attend(att_query, att_keys, att_values, map_lambda, diff_gain)
    retained = retain(ret_query, ret_keys, ret_values, decay_rate, state_gain)
    joined = jnp.concatenate([attended, retained], axis=1)
    diff_width = attended.shape[1]
    ret_width = retained.shape[1]
    tp_count = lax.axis_size("tp")
    tp_index = lax.axis_index("tp")
    own_rows = jnp.concatenate(
        [
            lax.dynamic_slice_in_dim(out_weight, tp_index * diff_width, diff_width, 0),
            lax.dynamic_slice_in_dim(
                out_weight, tp_count * diff_width + tp_index * ret_width, ret_width, 0
            ),
        ],
        axis=0,
    )
    output = lax.psum_scatter(
        jnp.dot(joined, own_rows, preferred_element_type=jnp.float32).astype(jnp.bfloat16),
        "tp",
        scatter_dimension=0,
        tiled=True,
    )
    return output[None]


def row_product(a, b):
    return lax.dot_general(a, b, (((1,), (1,)), ((), ())), preferred_element_type=jnp.float32)


MESH = pl.DeviceIdType.MESH


def greet(peers):
    barrier = pltpu.get_barrier_semaphore()
    count = 0
    for peer, present in peers:
        if present is None:
            pl.semaphore_signal(barrier, inc=1, device_id=peer, device_id_type=MESH)
            count = count + 1
        else:

            @pl.when(present)
            def _():
                pl.semaphore_signal(barrier, inc=1, device_id=peer, device_id_type=MESH)

            count = count + jnp.where(present, 1, 0)
    pl.semaphore_wait(barrier, count)


def layer_kernel(
    line,
    parts,
    tokens,
    gain,
    w0,
    w1,
    w2,
    w3,
    w4,
    w5,
    lam_ref,
    dgain_ref,
    rate_ref,
    sgain_ref,
    out_weight,
    result,
    seq,
    weight,
    proj,
    mine,
    joined,
    held,
    state,
    total,
    local_sem,
    held_sem,
    wsend,
    wrecv,
    lsend,
    lrecv,
    psend,
    precv,
    osend,
    orecv,
):
    f32, bf16 = jnp.float32, jnp.bfloat16
    weights = (w0, w1, w2, w3, w4, w5)
    kinds = len(weights)
    half_kinds = kinds // 2
    z, f, c = lax.axis_index("sp"), lax.axis_index("fs"), lax.axis_index("tp")
    block, half = tokens.shape
    piece = block // parts
    depth = w0.shape[0]
    width = weight.shape[1] // kinds
    rows_out = result.shape[0]
    me = c * line + z
    near = ({"fs": f ^ 1}, {"fs": f ^ 2})
    whose = (f ^ 1, f ^ 2, f ^ 3)
    greet(
        [
            (near[0], None),
            (near[1], None),
            ({"tp": 1 - c}, None),
            ({"sp": jnp.minimum(z + 1, line - 1)}, z + 1 < line),
            ({"sp": jnp.maximum(z - 1, 0)}, z > 0),
        ]
    )

    def held_at(b, side, q):
        return seq.at[
            pl.ds(pl.multiple_of(b * block + q * piece, piece), piece),
            pl.ds(pl.multiple_of(side * half, half), half),
        ]

    def own_tokens(q):
        return tokens.at[q * piece : (q + 1) * piece, :]

    def stored(owner, kind):
        return weight.at[
            pl.ds(pl.multiple_of(owner * depth, depth), depth), kind * width : (kind + 1) * width
        ]

    def slot(e):
        up = (e - 1) % 2 == 0
        s = (e - 1) // 2
        return z - 1 - s if up else z + 1 + s

    def along(e, b, q, source=None):
        target = z + 1 if (e - 1) % 2 == 0 else z - 1
        return pltpu.make_async_remote_copy(
            src_ref=held_at(b, c, q) if source is None else source,
            dst_ref=held_at(b, c, q),
            send_sem=lsend.at[e, q],
            recv_sem=lrecv.at[e, q],
            device_id={"sp": jnp.clip(target, 0, line - 1)},
            device_id_type=MESH,
        ), (target >= 0) & (target < line)

    def across(e, b, side, q, source=None):
        return pltpu.make_async_remote_copy(
            src_ref=held_at(b, side, q) if source is None else source,
            dst_ref=held_at(b, side, q),
            send_sem=psend.at[e, q],
            recv_sem=precv.at[e, q],
            device_id={"tp": 1 - c},
            device_id_type=MESH,
        )

    def own_columns(kind):
        return weights[kind].at[:, pl.ds(pl.multiple_of(z * width, width), width)]

    def spread(way, kind, source, owner, index):
        return pltpu.make_async_remote_copy(
            src_ref=source,
            dst_ref=stored(owner, kind),
            send_sem=wsend.at[way, index],
            recv_sem=wrecv.at[2 if index >= kinds else way, kind],
            device_id=near[way],
            device_id_type=MESH,
        )

    def arrived(relation, kind):
        pltpu.make_async_remote_copy(
            src_ref=stored(whose[relation], kind),
            dst_ref=stored(whose[relation], kind),
            send_sem=wsend.at[0, kind],
            recv_sem=wrecv.at[relation, kind],
            device_id=near[0],
            device_id_type=MESH,
        ).wait_recv()

    for q in range(parts):
        for e in (1, 2):
            copy, present = along(e, z, q, own_tokens(q))

            @pl.when(present)
            def _():
                copy.start()

    sends = []
    for turn in range(kinds):
        for way in range(2):
            kind = (turn + way * half_kinds) % kinds
            copy = spread(way, kind, own_columns(kind), f, kind)
            copy.start()
            sends.append(copy)
    locals_ = []
    for q in range(parts):
        across(0, z, c, q, own_tokens(q)).start()
        locals_.append(
            pltpu.make_async_copy(own_tokens(q), held_at(z, c, q), local_sem.at[kinds + q])
        )
    for kind in range(kinds):
        locals_.append(pltpu.make_async_copy(own_columns(kind), stored(f, kind), local_sem.at[kind]))
    for copy in locals_:
        copy.start()

    def relay(turn):
        for way in range(2):
            kind = turn + way * half_kinds
            arrived(way, kind)
            copy = spread(1 - way, kind, stored(whose[way], kind), whose[way], kinds + turn)
            copy.start()
            sends.append(copy)

    def take(s, q):
        for e in (1 + 2 * s, 2 + 2 * s):
            b = slot(e)

            @pl.when((b >= 0) & (b < line))
            def _():
                copy, _ = along(e, b, q)
                copy.wait_recv()
                if s + 1 < line - 1:
                    onward, present = along(e + 2, b, q)

                    @pl.when(present)
                    def _():
                        onward.start()

                across(e, b, c, q).start()

    def fetch(index):
        source = index // 2
        kind = index % 2
        first = kind * (out_weight.shape[0] // 2) + source * width
        return pltpu.make_async_copy(
            out_weight.at[first : first + width, :],
            held.at[source, kind * width : (kind + 1) * width, :],
            held_sem.at[index],
        )

    fetches = [fetch(index) for index in range(2 * joined.shape[0])]
    early = [(s, q) for s in range(line - 2) for q in range(parts)]
    for turn in range(half_kinds):
        relay(turn)
        if turn == 0:
            for copy in fetches:
                copy.start()
        elif early:
            take(*early.pop(0))
    for s, q in early:
        take(s, q)
    for copy in locals_:
        copy.wait()
    for kind in range(kinds):
        for relation in range(3):
            if relation == 2 or not (relation * half_kinds <= kind < (relation + 1) * half_kinds):
                arrived(relation, kind)

    def process(b):
        rows = pl.ds(pl.multiple_of(b * block, block), block)
        x = seq[rows, :].astype(f32)
        scaled = x * lax.rsqrt(jnp.mean(x * x, axis=1, keepdims=True) + epsilon)
        normed = (scaled * gain[...]).astype(bf16)
        proj[rows, :] = jnp.dot(normed, weight[...], preferred_element_type=f32).astype(bf16)

    def handle(e, carry):
        up = (e - 1) % 2 == 0
        s = (e - 1) // 2
        b = jnp.where(e == 0, z, jnp.where(up, z - 1 - s, z + 1 + s))

        @pl.when((b >= 0) & (b < line))
        def _():
            for q in range(parts):
                across(e, b, 1 - c, q).wait_recv()
            process(b)

        return carry

    row = lax.broadcasted_iota(jnp.int32, (block, block), 0)
    col = lax.broadcasted_iota(jnp.int32, (block, block), 1)
    lane = lax.broadcasted_iota(jnp.int32, (block, 2 * DK), 1)
    position = lax.broadcasted_iota(jnp.int32, (block, 1), 0).astype(f32)
    own_lanes = pl.ds(pl.multiple_of(z * DV, DV), DV)

    def part(kind, first, count):
        return proj[first : first + count, kind * DV : kind * DV + DV]

    def mix(b):
        first = b * block
        causal = col <= row
        lam = lam_ref[z]
        rate = rate_ref[z]
        query = part(0, first, block) * jnp.asarray(DK ** (-0.5), bf16)
        averaged = []
        for which in range(2):
            own = jnp.where((lane >= DK) == bool(which), query, jnp.zeros_like(query))
            near_scores = jnp.where(causal, row_product(own, part(1, first, block)), masked_score)
            peak = jnp.max(near_scores, axis=1, keepdims=True)
            if first:
                far = row_product(own, part(1, 0, first))
                peak = jnp.maximum(peak, jnp.max(far, axis=1, keepdims=True))
            near_scores = jnp.exp(near_scores - peak)
            count = jnp.sum(near_scores, axis=1, keepdims=True)
            summed = jnp.dot(
                near_scores.astype(bf16), part(2, first, block), preferred_element_type=f32
            )
            if first:
                far = jnp.exp(far - peak)
                count = count + jnp.sum(far, axis=1, keepdims=True)
                summed = summed + jnp.dot(
                    far.astype(bf16), part(2, 0, first), preferred_element_type=f32
                )
            averaged.append(summed / count)
        differ = averaged[0] - lam * averaged[1]
        scaled = differ * lax.rsqrt(jnp.mean(differ * differ, axis=1, keepdims=True) + epsilon)
        mine[first : first + block, :DV] = (
            scaled * (dgain_ref[:, own_lanes] * branch_scale)
        ).astype(bf16)
        ret_query = part(3, first, block)
        ret_keys = part(4, first, block)
        ret_values = part(5, first, block)
        within = jnp.where(causal, jnp.exp(-rate * jnp.maximum(row - col, 0).astype(f32)), 0.0)
        local = (row_product(ret_query, ret_keys) * within).astype(bf16)
        mixed = jnp.dot(local, ret_values, preferred_element_type=f32)
        if first:
            mixed = mixed + jnp.exp(-rate * (position + 1.0)) * jnp.dot(
                ret_query, state[...].astype(bf16), preferred_element_type=f32
            )
        if b + 1 < line:
            decayed = (ret_keys.astype(f32) * jnp.exp(-rate * (block - 1.0 - position))).astype(bf16)
            update = lax.dot_general(
                decayed, ret_values, (((0,), (0,)), ((), ())), preferred_element_type=f32
            )
            if first:
                update = state[...] * jnp.exp(jnp.full((1, DR), -block, f32) * rate) + update
            state[...] = update
        scaled = mixed * lax.rsqrt(jnp.mean(mixed * mixed, axis=1, keepdims=True) + epsilon)
        mine[first : first + block, DV:] = (scaled * sgain_ref[:, own_lanes]).astype(bf16)

    def mine_rows(b, side):
        return mine.at[pl.ds(pl.multiple_of(b * block + side * rows_out, rows_out), rows_out), :]

    def deliver(b, turn):
        side = c if turn == 0 else 1 - c
        return pltpu.make_async_remote_copy(
            src_ref=mine_rows(b, side),
            dst_ref=joined.at[me],
            send_sem=osend.at[b, turn],
            recv_sem=orecv.at[me],
            device_id={"sp": b, "tp": side},
            device_id_type=MESH,
        )

    def give(b):
        deliver(b, 1).start()

        @pl.when(z != b)
        def _():
            deliver(b, 0).start()

        @pl.when(z == b)
        def _():
            joined[me] = mine_rows(b, c)[...]

    last = 2 * line - 3
    lax.fori_loop(0, last, handle, 0)

    def phase(t, carry):
        @pl.when(t == 1)
        def _():
            for q in range(parts):
                take(line - 2, q)
            lax.fori_loop(last, last + 2, handle, 0)

        for b in range(line):
            late = z == line - 1
            if b == line - 1:
                late = late | (z == 0)

            @pl.when(late == (t == 1))
            def _():
                mix(b)
                give(b)

        return carry

    lax.fori_loop(0, 2, phase, 0)

    for copy in fetches:
        copy.wait()
    order = [s for s in range(1, line - 1)] + [0, line - 1]
    for index, source in enumerate(order):
        for turn in range(2):
            side = c if turn == 0 else 1 - c
            where = side * line + source

            @pl.when(where != me)
            def _():
                pltpu.make_async_remote_copy(
                    src_ref=joined.at[where],
                    dst_ref=joined.at[where],
                    send_sem=osend.at[0, 0],
                    recv_sem=orecv.at[where],
                    device_id={"tp": 1 - c},
                    device_id_type=MESH,
                ).wait_recv()

            product = jnp.dot(joined[where], held[where], preferred_element_type=f32)
            if index == 0 and turn == 0:
                total[...] = product
            elif index < line - 1 or turn == 0:
                total[...] += product
            else:
                result[...] = (total[...] + product).astype(bf16)

    for copy in sends:
        copy.wait_send()
    for q in range(parts):
        across(0, z, c, q, own_tokens(q)).wait_send()
        for e in (1, 2):
            copy, present = along(e, z, q, own_tokens(q))

            @pl.when(present)
            def _():
                copy.wait_send()

        for s in range(line - 1):
            for e in (1 + 2 * s, 2 + 2 * s):
                b = slot(e)

                @pl.when((b >= 0) & (b < line))
                def _():
                    across(e, b, c, q).wait_send()
                    if s + 1 < line - 1:
                        onward, present = along(e + 2, b, q)

                        @pl.when(present)
                        def _():
                            onward.wait_send()

    for b in range(line):
        deliver(b, 1).wait_send()

        @pl.when(z != b)
        def _():
            deliver(b, 0).wait_send()


def whole_layer(tokens, norm_gain, weights, map_lambda, diff_gain, decay_rate, state_gain, out_weight, line, pair):
    block, half = tokens.shape
    kinds = len(weights)
    model = norm_gain.shape[0]
    parts = 2
    rows = block // pair
    count = line * pair
    anywhere = pl.BlockSpec(memory_space=pl.ANY)
    vmem = pl.BlockSpec(memory_space=pltpu.VMEM)
    smem = pl.BlockSpec(memory_space=pltpu.SMEM)
    events = 2 * line - 1
    dma = pltpu.SemaphoreType.DMA
    bf16 = jnp.bfloat16
    return pl.pallas_call(
        functools.partial(layer_kernel, line, parts),
        out_shape=jax.ShapeDtypeStruct((rows, out_weight.shape[1]), bf16),
        in_specs=[anywhere, vmem] + [anywhere] * kinds + [smem, vmem, smem, vmem, anywhere],
        out_specs=vmem,
        scratch_shapes=[
            pltpu.VMEM((line * block, model), bf16),
            pltpu.VMEM((model, kinds * DV), bf16),
            pltpu.VMEM((line * block, kinds * DV), bf16),
            pltpu.VMEM((line * block, 2 * DV), bf16),
            pltpu.VMEM((count, rows, 2 * DV), bf16),
            pltpu.VMEM((count, 2 * DV, out_weight.shape[1]), bf16),
            pltpu.VMEM((DR, DR), jnp.float32),
            pltpu.VMEM((rows, out_weight.shape[1]), jnp.float32),
            dma((kinds + parts,)),
            dma((2 * count,)),
            dma((2, kinds + kinds // 2)),
            dma((3, kinds)),
            dma((events, parts)),
            dma((events, parts)),
            dma((events, parts)),
            dma((events, parts)),
            dma((line, pair)),
            dma((count,)),
        ],
        compiler_params=pltpu.CompilerParams(
            collective_id=0, has_side_effects=True, vmem_limit_bytes=65000 * 1024
        ),
    )(
        tokens,
        norm_gain[None],
        *weights,
        map_lambda,
        diff_gain[None],
        decay_rate,
        state_gain[None],
        out_weight,
    )


def body(tokens, norm_gain, *rest):
    weights, (map_lambda, diff_gain, decay_rate, state_gain, out_weight) = rest[:6], rest[6:]
    line = lax.axis_size("sp")
    pair = lax.axis_size("tp")
    local = map_lambda.shape[0]
    if local != line or decay_rate.shape[0] != local or lax.axis_size("fs") != 4 or pair != 2:
        return spread_body(tokens, norm_gain, *rest)
    return whole_layer(
        tokens[0],
        norm_gain,
        weights,
        map_lambda,
        diff_gain,
        decay_rate,
        state_gain,
        out_weight,
        line,
        pair,
    )[None]


def solution(mesh):
    placed = (
        P("fs", "sp", "tp"),
        P(),
        P("fs", "tp"),
        P("fs", "tp"),
        P("fs", "tp"),
        P("fs", "tp"),
        P("fs", "tp"),
        P("fs", "tp"),
        P("tp"),
        P("tp"),
        P("tp"),
        P("tp"),
        P(),
    )
    return jax.shard_map(
        body, mesh=mesh, in_specs=placed, out_specs=P("fs", ("sp", "tp"), None), check_vma=False
    )
```

```python
import functools

import jax
import jax.numpy as jnp
from jax import lax
from jax.experimental import pallas as pl
from jax.experimental.pallas import tpu as pltpu
from jax.sharding import PartitionSpec as P

DK = 64
DV = 128
DR = 128


epsilon = 1e-05
branch_scale = 0.8
masked_score = -1e30


def from_behind(x, axis, by):
    size = lax.axis_size(axis)
    pairs = [(i, i + by) for i in range(size) if 0 <= i + by < size]
    return lax.ppermute(x, axis, pairs)


def entering(x, axis, join, neutral):
    place = lax.axis_index(axis)
    gathered = jax.tree.map(
        lambda a, kind: lax.all_gather(a.astype(kind), axis), x, (jnp.bfloat16, jnp.bfloat16)
    )
    state = jax.tree.map(lambda a, e: jnp.zeros_like(a) + jnp.asarray(e, a.dtype), x, neutral)

    def one(turn, state):
        return join(
            state,
            jax.tree.map(
                lambda a, own: lax.dynamic_index_in_dim(a, turn, 0, False).astype(own.dtype),
                gathered,
                x,
            ),
        )

    return lax.fori_loop(0, place, one, state)


def attend(att_query, att_keys, att_values, map_lambda, diff_gain):
    tok_rows = att_query.shape[0]
    head_count = map_lambda.shape[0]
    key_width = att_keys.shape[1]
    query_heads = att_query.reshape(tok_rows, head_count, 2, DK)
    sp_index = lax.axis_index("sp")
    query_place = sp_index * tok_rows + jnp.arange(tok_rows)
    score_scale = DK ** (-0.5)

    def absorb_block(running, inputs):
        key_block, key_place = inputs
        key_heads = key_block[:, :key_width].reshape(tok_rows, head_count, 2, DK)
        value_heads = key_block[:, key_width:].reshape(tok_rows, head_count, DV)
        scores = (
            jnp.einsum(
                "qhmd,khmd->mhqk", query_heads, key_heads, preferred_element_type=jnp.float32
            )
            * score_scale
        )
        causal = key_place[None, :] <= query_place[:, None]
        row_peak, totals, summed = running
        new_peak = jnp.maximum(row_peak, jnp.max(jnp.where(causal, scores, masked_score), axis=-1))
        weights = jnp.where(causal, jnp.exp(scores - new_peak[..., None]), 0.0)
        factor = jnp.exp(row_peak - new_peak)
        totals = totals * factor + jnp.sum(weights, axis=-1)
        summed = summed * factor[..., None] + jnp.einsum(
            "mhqk,khv->mhqv",
            weights.astype(jnp.bfloat16),
            value_heads,
            preferred_element_type=jnp.float32,
        )
        return ((new_peak, totals, summed), None)

    def absorb(running, pieces, first_row):
        piece_rows = pieces.shape[0]
        stacked = pieces.reshape(piece_rows // tok_rows, tok_rows, pieces.shape[1])
        places = (first_row + jnp.arange(piece_rows)).reshape(piece_rows // tok_rows, tok_rows)
        return lax.scan(absorb_block, running, (stacked, places))[0]

    starting = (
        jnp.full((2, head_count, tok_rows), masked_score, jnp.float32),
        jnp.zeros((2, head_count, tok_rows), jnp.float32),
        jnp.zeros((2, head_count, tok_rows, DV), jnp.float32),
    )
    joined_kv = jnp.concatenate([att_keys, att_values], axis=1)
    first_state = absorb(starting, joined_kv, sp_index * tok_rows)

    def relay_step(step_index, relay_state):
        running, moving = relay_state
        moving = from_behind(moving, "sp", 1)
        first_row = (sp_index - step_index) * tok_rows
        running = lax.cond(
            first_row >= 0,
            lambda holding: absorb(holding, moving, first_row),
            lambda holding: holding,
            running,
        )
        return (running, moving)

    running, _ = lax.fori_loop(1, lax.axis_size("sp"), relay_step, (first_state, joined_kv))
    row_peak, totals, summed = running
    averaged = summed / totals[..., None]
    differ = averaged[0] - map_lambda[:, None, None] * averaged[1]
    normed = differ * lax.rsqrt(jnp.mean(differ * differ, axis=-1, keepdims=True) + epsilon)
    normed = normed * diff_gain.reshape(head_count, 1, DV) * branch_scale
    return normed.transpose(1, 0, 2).reshape(tok_rows, head_count * DV).astype(jnp.bfloat16)


def retain(ret_query, ret_keys, ret_values, decay_rate, state_gain):
    tok_rows = ret_query.shape[0]
    head_count = decay_rate.shape[0]
    query_heads = ret_query.reshape(tok_rows, head_count, DR)
    key_heads = ret_keys.reshape(tok_rows, head_count, DR)
    value_heads = ret_values.reshape(tok_rows, head_count, DR)
    position = jnp.arange(tok_rows).astype(jnp.float32)
    distance = position[:, None] - position[None, :]
    decay_col = decay_rate[:, None, None]
    within = jnp.where(distance >= 0, jnp.exp(-decay_col * jnp.maximum(distance, 0.0)), 0.0)
    local_scores = (
        jnp.einsum("qhd,khd->hqk", query_heads, key_heads, preferred_element_type=jnp.float32)
        * within
    )
    intra_out = jnp.einsum(
        "hqk,khv->hqv",
        local_scores.astype(jnp.bfloat16),
        value_heads,
        preferred_element_type=jnp.float32,
    )
    key_decayed = key_heads.astype(jnp.float32) * jnp.exp(
        -decay_rate[None, :, None] * (tok_rows - 1.0 - position)[:, None, None]
    )
    own_state = jnp.einsum(
        "khd,khv->hdv",
        key_decayed,
        value_heads.astype(jnp.float32),
        precision=lax.Precision.HIGHEST,
    )
    block_decay = jnp.exp(-decay_rate * tok_rows)

    def link_states(earlier, later):
        return (earlier[0] * later[1][:, None, None] + later[0], earlier[1] * later[1])

    identity = (jnp.zeros_like(own_state), jnp.ones_like(block_decay))
    incoming, _ = entering((own_state, block_decay), "sp", link_states, identity)
    carried = jnp.einsum(
        "qhd,hdv->hqv", query_heads.astype(jnp.float32), incoming, precision=lax.Precision.HIGHEST
    )
    carried = carried * jnp.exp(-decay_col * (position + 1.0)[None, :, None])
    combined = intra_out + carried
    normed = combined * lax.rsqrt(jnp.mean(combined * combined, axis=-1, keepdims=True) + epsilon)
    normed = normed * state_gain.reshape(head_count, 1, DR)
    return normed.transpose(1, 0, 2).reshape(tok_rows, head_count * DR).astype(jnp.bfloat16)


def spread_body(
    tokens,
    norm_gain,
    query_weight,
    key_weight,
    value_weight,
    state_query,
    state_key,
    state_value,
    map_lambda,
    diff_gain,
    decay_rate,
    state_gain,
    out_weight,
):
    gathered = lax.all_gather(tokens[0], "tp", axis=1, tiled=True)
    tok_float = gathered.astype(jnp.float32)
    normed = tok_float * lax.rsqrt(
        jnp.mean(tok_float * tok_float, axis=-1, keepdims=True) + epsilon
    )
    normed = (normed * norm_gain).astype(jnp.bfloat16)
    pieces = (
        lax.all_gather(query_weight, "fs", axis=0, tiled=True),
        lax.all_gather(key_weight, "fs", axis=0, tiled=True),
        lax.all_gather(value_weight, "fs", axis=0, tiled=True),
        lax.all_gather(state_query, "fs", axis=0, tiled=True),
        lax.all_gather(state_key, "fs", axis=0, tiled=True),
        lax.all_gather(state_value, "fs", axis=0, tiled=True),
    )
    projected = tuple(
        (jnp.dot(normed, row_block, preferred_element_type=jnp.float32) for row_block in pieces)
    )
    att_query, att_keys, att_values, ret_query, ret_keys, ret_values = (
        member.astype(jnp.bfloat16) for member in projected
    )
    attended = attend(att_query, att_keys, att_values, map_lambda, diff_gain)
    retained = retain(ret_query, ret_keys, ret_values, decay_rate, state_gain)
    joined = jnp.concatenate([attended, retained], axis=1)
    diff_width = attended.shape[1]
    ret_width = retained.shape[1]
    tp_count = lax.axis_size("tp")
    tp_index = lax.axis_index("tp")
    own_rows = jnp.concatenate(
        [
            lax.dynamic_slice_in_dim(out_weight, tp_index * diff_width, diff_width, 0),
            lax.dynamic_slice_in_dim(
                out_weight, tp_count * diff_width + tp_index * ret_width, ret_width, 0
            ),
        ],
        axis=0,
    )
    output = lax.psum_scatter(
        jnp.dot(joined, own_rows, preferred_element_type=jnp.float32).astype(jnp.bfloat16),
        "tp",
        scatter_dimension=0,
        tiled=True,
    )
    return output[None]


def row_product(a, b):
    return lax.dot_general(a, b, (((1,), (1,)), ((), ())), preferred_element_type=jnp.float32)


MESH = pl.DeviceIdType.MESH


def greet(peers):
    barrier = pltpu.get_barrier_semaphore()
    count = 0
    for peer, present in peers:
        if present is None:
            pl.semaphore_signal(barrier, inc=1, device_id=peer, device_id_type=MESH)
            count = count + 1
        else:

            @pl.when(present)
            def _():
                pl.semaphore_signal(barrier, inc=1, device_id=peer, device_id_type=MESH)

            count = count + jnp.where(present, 1, 0)
    pl.semaphore_wait(barrier, count)


def layer_kernel(
    line,
    parts,
    tokens,
    gain_in,
    w0,
    w1,
    w2,
    w3,
    w4,
    w5,
    lam_in,
    dgain_in,
    rate_in,
    sgain_in,
    out_weight,
    result,
    gains,
    lam_ref,
    rate_ref,
    seq,
    normal,
    weight,
    proj,
    mine,
    joined,
    held,
    state,
    total,
    local_sem,
    held_sem,
    wsend,
    wrecv,
    lsend,
    lrecv,
    psend,
    precv,
    osend,
    orecv,
):
    f32, bf16 = jnp.float32, jnp.bfloat16
    weights = (w0, w1, w2, w3, w4, w5)
    kinds = len(weights)
    half_kinds = kinds // 2
    early_parts = parts // 2
    events = 2 * line - 1
    z, f, c = lax.axis_index("sp"), lax.axis_index("fs"), lax.axis_index("tp")
    block, half = tokens.shape
    piece = block // parts
    depth = w0.shape[0]
    width = weight.shape[1] // kinds
    rows_out = result.shape[0]
    model = seq.shape[1]
    me = c * line + z
    near = ({"fs": f ^ 1}, {"fs": f ^ 2})
    whose = (f ^ 1, f ^ 2, f ^ 3)
    greet(
        [
            (near[0], None),
            (near[1], None),
            ({"tp": 1 - c}, None),
            ({"sp": jnp.minimum(z + 1, line - 1)}, z + 1 < line),
            ({"sp": jnp.maximum(z - 1, 0)}, z > 0),
        ]
    )

    def held_at(b, side, q):
        return seq.at[
            pl.ds(pl.multiple_of(b * block + q * piece, piece), piece),
            pl.ds(pl.multiple_of(side * half, half), half),
        ]

    def whole(b, side):
        return seq.at[
            pl.ds(pl.multiple_of(b * block, block), block),
            pl.ds(pl.multiple_of(side * half, half), half),
        ]

    def own_tokens(q):
        return tokens.at[q * piece : (q + 1) * piece, :]

    def column(kind):
        return (2 * (kind % half_kinds) + kind // half_kinds) * width

    def stored(owner, kind):
        return weight.at[
            pl.ds(pl.multiple_of(owner * depth, depth), depth), column(kind) : column(kind) + width
        ]

    def slot(e):
        up = (e - 1) % 2 == 0
        s = (e - 1) // 2
        return z - 1 - s if up else z + 1 + s

    def along(e, b, q, source=None):
        target = z + 1 if (e - 1) % 2 == 0 else z - 1
        return pltpu.make_async_remote_copy(
            src_ref=held_at(b, c, q) if source is None else source,
            dst_ref=held_at(b, c, q),
            send_sem=lsend.at[e],
            recv_sem=lrecv.at[e, q],
            device_id={"sp": jnp.clip(target, 0, line - 1)},
            device_id_type=MESH,
        ), (target >= 0) & (target < line)

    def across(e, b, side, q, source=None):
        return pltpu.make_async_remote_copy(
            src_ref=held_at(b, side, q) if source is None else source,
            dst_ref=held_at(b, side, q),
            send_sem=psend.at[e],
            recv_sem=precv.at[e],
            device_id={"tp": 1 - c},
            device_id_type=MESH,
        )

    def all_along(e):
        return pltpu.make_async_remote_copy(
            src_ref=tokens,
            dst_ref=whole(z, c),
            send_sem=lsend.at[e],
            recv_sem=lrecv.at[e, 0],
            device_id={"sp": z ^ 1},
            device_id_type=MESH,
        )

    def all_across(e, b):
        return pltpu.make_async_remote_copy(
            src_ref=whole(b, 1 - c),
            dst_ref=whole(b, 1 - c),
            send_sem=psend.at[e],
            recv_sem=precv.at[e],
            device_id={"tp": 1 - c},
            device_id_type=MESH,
        )

    def own_columns(kind):
        return weights[kind].at[:, pl.ds(pl.multiple_of(z * width, width), width)]

    def arrival(relation, kind):
        return kind if relation == kind // half_kinds else kinds + kind % half_kinds

    def spread(way, kind, source, owner, index):
        return pltpu.make_async_remote_copy(
            src_ref=source,
            dst_ref=stored(owner, kind),
            send_sem=wsend,
            recv_sem=wrecv.at[arrival(2 if index >= kinds else way, kind)],
            device_id=near[way],
            device_id_type=MESH,
        )

    def arrived(relation, kind):
        pltpu.make_async_remote_copy(
            src_ref=stored(whose[relation], kind),
            dst_ref=stored(whose[relation], kind),
            send_sem=wsend,
            recv_sem=wrecv.at[arrival(relation, kind)],
            device_id=near[0],
            device_id_type=MESH,
        ).wait_recv()

    def push(e, q, when=True):
        copy, present = along(e, z, q, own_tokens(q))

        @pl.when(present & when)
        def _():
            copy.start()

    def scatter(pair):
        for kind in (pair, pair + half_kinds):
            for way in range(2):
                spread(way, kind, own_columns(kind), f, kind).start()

    for q in range(parts):
        push(1, q, z >= 0 if q < early_parts else z == 0)
        push(2, q)
    scatter(0)
    locals_ = []
    for q in range(parts):
        across(0, z, c, q, own_tokens(q)).start()
    locals_.append(pltpu.make_async_copy(tokens, whole(z, c), local_sem.at[0]))
    scatter(1)
    for kind in range(kinds):
        locals_.append(pltpu.make_async_copy(own_columns(kind), stored(f, kind), local_sem.at[1]))
    spots = ((gain_in, 0), (dgain_in, model), (sgain_in, model + dgain_in.shape[1]))
    for source, first in spots:
        locals_.append(
            pltpu.make_async_copy(
                source, gains.at[:, first : first + source.shape[1]], local_sem.at[2]
            )
        )
    locals_.append(pltpu.make_async_copy(lam_in, lam_ref, local_sem.at[3]))
    locals_.append(pltpu.make_async_copy(rate_in, rate_ref, local_sem.at[4]))
    for copy in locals_:
        copy.start()

    def relay(turn):
        for way in range(2):
            kind = turn + way * half_kinds
            arrived(way, kind)
            spread(1 - way, kind, stored(whose[way], kind), whose[way], kinds + turn).start()

    def complete(turn):
        landed = weight.at[: 2 * depth, 2 * turn * width : 2 * (turn + 1) * width]
        pltpu.make_async_remote_copy(
            src_ref=landed,
            dst_ref=landed,
            send_sem=wsend,
            recv_sem=wrecv.at[kinds + turn],
            device_id=near[0],
            device_id_type=MESH,
        ).wait_recv()

    def serve(e, q, when):
        b = slot(e)

        @pl.when((b >= 0) & (b < line) & when)
        def _():
            copy, _ = along(e, b, q)
            copy.wait_recv()
            if (e - 1) // 2 + 1 < line - 1:
                onward, present = along(e + 2, b, q)

                @pl.when(present)
                def _():
                    onward.start()

            across(e, b, c, q).start()

    def at_slot(k):
        for s in range(line - 1):
            for q in range(parts):
                if q < early_parts:
                    if k == s * early_parts + q:
                        serve(1 + 2 * s, q, z > s)
                else:
                    for other in range(s + 1, line):
                        if k == (2 * other - 4 - s) * early_parts + parts + q:
                            serve(1 + 2 * s, q, z == other)
        serve(2 + 2 * (k // parts), k % parts, z >= 0)
        if k % parts == parts - 1 and k // parts < line - 2:
            for q in range(early_parts, parts):
                push(1, q, z == k // parts + 1)

    def fetch(index):
        source = index // 2
        kind = index % 2
        first = kind * (out_weight.shape[0] // 2) + source * width
        return pltpu.make_async_copy(
            out_weight.at[first : first + width, :],
            held.at[source, kind * width : (kind + 1) * width, :],
            held_sem,
        )

    fetches = [fetch(index) for index in range(2 * joined.shape[0])]

    def block_of(e):
        s = (e - 1) // 2
        return jnp.where(e == 0, z, jnp.where((e - 1) % 2 == 0, z - 1 - s, z + 1 + s))

    def rows_of(b):
        return pl.ds(pl.multiple_of(b * block, block), block)

    def normalize(e, b):
        all_across(e, b).wait_recv()
        x = seq[rows_of(b), :].astype(f32)
        scaled = x * lax.rsqrt(jnp.mean(x * x, axis=1, keepdims=True) + epsilon)
        normal[rows_of(b), :] = (scaled * gains[:, :model]).astype(bf16)

    def project(b, pair):
        columns = pl.ds(pl.multiple_of(pair * 2 * width, 2 * width), 2 * width)
        proj[rows_of(b), columns] = jnp.dot(
            normal[rows_of(b), :], weight[:, columns], preferred_element_type=f32
        ).astype(bf16)

    def soon(e, b):
        return (e == 0) | (((e == 2) | ((e == 1) & (z == 1))) & (b < line))

    def late(e):
        return ((z == line - 1) & (e % 2 == 1) & (e < events - 2)) | ((z == 0) & (e == events - 1))

    def first_pair(chosen):
        def one(e, carry):
            b = block_of(e)

            @pl.when((b >= 0) & (b < line) & chosen(e, b))
            def _():
                normalize(e, b)
                project(b, 0)

            return carry

        return one

    def next_pair(pair):
        def one(b, carry):
            @pl.when(
                ((z > 0) | (b < line - 1)) & ((z < line - 1) | (b == 0) | (b == line - 1))
            )
            def _():
                project(b, pair)

            return carry

        lax.fori_loop(0, line, one, 0)

    middle = parts + 1
    early_slots = parts * (line - 2)
    for k in range(early_slots):
        at_slot(k)
        if k == 0:
            relay(0)
            scatter(2)
            for copy in fetches:
                copy.start()
        if k == 2:
            relay(1)
        if k == middle:
            relay(2)
        if k == parts:
            for copy in locals_[:1] + locals_[-2:]:
                copy.wait()
            mine_rows_in = weight.at[pl.ds(pl.multiple_of(f * depth, depth), depth), :]
            pltpu.make_async_copy(mine_rows_in, mine_rows_in, local_sem.at[1]).wait()
            pltpu.make_async_copy(gains, gains, local_sem.at[2]).wait()
            complete(0)
            lax.fori_loop(0, 3, first_pair(soon), 0)
    complete(1)
    lax.fori_loop(1, events, first_pair(lambda e, b: ~soon(e, b) & ~late(e)), 0)
    next_pair(1)
    complete(2)
    next_pair(2)

    row = lax.broadcasted_iota(jnp.int32, (block, block), 0)
    col = lax.broadcasted_iota(jnp.int32, (block, block), 1)
    lane = lax.broadcasted_iota(jnp.int32, (block, 2 * DK), 1)
    position = lax.broadcasted_iota(jnp.int32, (block, 1), 0).astype(f32)

    def part(kind, first, count):
        return proj[first : first + count, column(kind) : column(kind) + DV]

    def mix(b):
        first = b * block
        causal = col <= row
        lam = lam_ref[z]
        rate = rate_ref[z]
        query = part(0, first, block) * jnp.asarray(DK ** (-0.5), bf16)
        averaged = []
        for which in range(2):
            own = jnp.where((lane >= DK) == bool(which), query, jnp.zeros_like(query))
            near_scores = jnp.where(causal, row_product(own, part(1, first, block)), masked_score)
            peak = jnp.max(near_scores, axis=1, keepdims=True)
            if first:
                far = row_product(own, part(1, 0, first))
                peak = jnp.maximum(peak, jnp.max(far, axis=1, keepdims=True))
            near_scores = jnp.exp(near_scores - peak)
            count = jnp.sum(near_scores, axis=1, keepdims=True)
            summed = jnp.dot(
                near_scores.astype(bf16), part(2, first, block), preferred_element_type=f32
            )
            if first:
                far = jnp.exp(far - peak)
                count = count + jnp.sum(far, axis=1, keepdims=True)
                summed = summed + jnp.dot(
                    far.astype(bf16), part(2, 0, first), preferred_element_type=f32
                )
            averaged.append(summed / count)
        differ = averaged[0] - lam * averaged[1]
        scaled = differ * lax.rsqrt(jnp.mean(differ * differ, axis=1, keepdims=True) + epsilon)
        mine[first : first + block, :DV] = (
            scaled * (gains[:, pl.ds(pl.multiple_of(model + z * DV, DV), DV)] * branch_scale)
        ).astype(bf16)
        ret_query = part(3, first, block)
        ret_keys = part(4, first, block)
        ret_values = part(5, first, block)
        within = jnp.where(causal, jnp.exp(-rate * jnp.maximum(row - col, 0).astype(f32)), 0.0)
        local = (row_product(ret_query, ret_keys) * within).astype(bf16)
        mixed = jnp.dot(local, ret_values, preferred_element_type=f32)
        if first:
            mixed = mixed + jnp.exp(-rate * (position + 1.0)) * jnp.dot(
                ret_query, state[...].astype(bf16), preferred_element_type=f32
            )
        if b + 1 < line:
            decayed = (ret_keys.astype(f32) * jnp.exp(-rate * (block - 1.0 - position))).astype(bf16)
            update = lax.dot_general(
                decayed, ret_values, (((0,), (0,)), ((), ())), preferred_element_type=f32
            )
            if first:
                update = state[...] * jnp.exp(jnp.full((1, DR), -block, f32) * rate) + update
            state[...] = update
        scaled = mixed * lax.rsqrt(jnp.mean(mixed * mixed, axis=1, keepdims=True) + epsilon)
        mine[first : first + block, DV:] = (scaled * gains[:, pl.ds(pl.multiple_of(model + dgain_in.shape[1] + z * DV, DV), DV)]).astype(bf16)

    def mine_rows(b, side):
        return mine.at[pl.ds(pl.multiple_of(b * block + side * rows_out, rows_out), rows_out), :]

    def deliver(b, h):
        return pltpu.make_async_remote_copy(
            src_ref=mine_rows(b, h),
            dst_ref=joined.at[me],
            send_sem=osend,
            recv_sem=orecv.at[me],
            device_id={"sp": b, "tp": h},
            device_id_type=MESH,
        )

    def own_place(b, h):
        return (z == b) & (c == h)

    def send(b, when):
        for h in range(2):

            @pl.when(when & ~own_place(b, h))
            def _():
                deliver(b, h).start()

    def give(b):
        if b == 0:
            send(b, z == 0)
        elif b == line - 1:
            send(b, (z == 0) | (z == line - 1))
        else:
            send(b, z >= 0)

        @pl.when(z == b)
        def _():
            joined[me] = mine_rows(b, c)[...]

    def last_token(end):
        if end == 0:
            return all_along(events - 1), z == 1
        return all_along(1), z == line - 2

    def phase(t, carry):
        @pl.when(t == line - 2)
        def _():
            for end in (0, line - 1):
                copy, here = last_token(end)

                @pl.when(here)
                def _():
                    copy.wait_send()

            send(0, z > 0)
            send(line - 1, (z > 0) & (z < line - 1))

        for turn in range(1, line - 1):

            @pl.when(t == turn)
            def _():
                for q in range(early_parts):
                    at_slot(early_slots + (turn - 1) * early_parts + q)

        @pl.when((t > 0) & ((z == line - 1) | ((z == 0) & (t == line - 2))))
        def _():
            b = jnp.where(z == 0, line - 1, t)
            e = jnp.where(z == 0, events - 1, 2 * (line - 2 - t) + 1)
            normalize(e, b)
            for pair in range(half_kinds):
                project(b, pair)

        for b in range(line):
            turn = jnp.where(z == line - 1, min(b, line - 2), 0)
            if b == line - 1:
                turn = jnp.where(z == 0, line - 2, turn)

            @pl.when(turn == t)
            def _():
                mix(b)
                give(b)

        return carry

    lax.fori_loop(0, line - 1, phase, 0)

    pltpu.make_async_copy(held, held, held_sem).wait()
    inner = [s for s in range(1, line - 1)]
    outer = (z == 0) | (z == line - 1)
    order = []
    for index in range(line):
        for_outer = ([0, line - 1] + inner)[index]
        for_inner = (inner + [0, line - 1])[index]
        order.append(jnp.where(outer, for_outer, for_inner))
    for index, source in enumerate(order):
        for turn in range(2):
            side = c if turn == 0 else 1 - c
            where = side * line + source

            @pl.when(where != me)
            def _():
                pltpu.make_async_remote_copy(
                    src_ref=joined.at[where],
                    dst_ref=joined.at[where],
                    send_sem=osend,
                    recv_sem=orecv.at[where],
                    device_id={"tp": 1 - c},
                    device_id_type=MESH,
                ).wait_recv()

            product = jnp.dot(joined[where], held[where], preferred_element_type=f32)
            if index == 0 and turn == 0:
                total[...] = product
            elif index < line - 1 or turn == 0:
                total[...] += product
            else:
                result[...] = (total[...] + product).astype(bf16)

    sent = weight.at[: 3 * depth, :]
    pltpu.make_async_remote_copy(
        src_ref=sent,
        dst_ref=sent,
        send_sem=wsend,
        recv_sem=wrecv.at[0],
        device_id=near[0],
        device_id_type=MESH,
    ).wait_send()
    for e in range(events):
        b = block_of(e)

        @pl.when((b >= 0) & (b < line))
        def _():
            all_across(e, b).wait_send()

        if e == 0:
            continue
        up = e % 2 == 1
        target = z + 1 if up else z - 1
        s = (e - 1) // 2
        source = z - s if up else z + s
        present = (target >= 0) & (target < line) & (source >= 0) & (source < line)
        if e == 1:
            present = present & (z != line - 2)
        if e == events - 1:
            present = present & (z != 1)

        @pl.when(present)
        def _():
            all_along(e).wait_send()

    gone = mine.at[: (2 * line - 1) * rows_out, :]
    pltpu.make_async_remote_copy(
        src_ref=gone,
        dst_ref=gone,
        send_sem=osend,
        recv_sem=orecv.at[0],
        device_id={"tp": 1 - c},
        device_id_type=MESH,
    ).wait_send()


def whole_layer(tokens, norm_gain, weights, map_lambda, diff_gain, decay_rate, state_gain, out_weight, line, pair):
    block, half = tokens.shape
    kinds = len(weights)
    model = norm_gain.shape[0]
    parts = 2
    rows = block // pair
    count = line * pair
    anywhere = pl.BlockSpec(memory_space=pl.ANY)
    vmem = pl.BlockSpec(memory_space=pltpu.VMEM)
    events = 2 * line - 1
    dma = pltpu.SemaphoreType.DMA
    bf16 = jnp.bfloat16
    return pl.pallas_call(
        functools.partial(layer_kernel, line, parts),
        out_shape=jax.ShapeDtypeStruct((rows, out_weight.shape[1]), bf16),
        in_specs=[anywhere] * (kinds + 7),
        out_specs=vmem,
        scratch_shapes=[
            pltpu.VMEM((1, model + diff_gain.shape[0] + state_gain.shape[0]), jnp.float32),
            pltpu.SMEM(map_lambda.shape, jnp.float32),
            pltpu.SMEM(decay_rate.shape, jnp.float32),
            pltpu.VMEM((line * block, model), bf16),
            pltpu.VMEM((line * block, model), bf16),
            pltpu.VMEM((model, kinds * DV), bf16),
            pltpu.VMEM((line * block, kinds * DV), bf16),
            pltpu.VMEM((line * block, 2 * DV), bf16),
            pltpu.VMEM((count, rows, 2 * DV), bf16),
            pltpu.VMEM((count, 2 * DV, out_weight.shape[1]), bf16),
            pltpu.VMEM((DR, DR), jnp.float32),
            pltpu.VMEM((rows, out_weight.shape[1]), jnp.float32),
            dma((5,)),
            dma,
            dma,
            dma((kinds + kinds // 2,)),
            dma((events,)),
            dma((events, parts)),
            dma((events,)),
            dma((events,)),
            dma,
            dma((count,)),
        ],
        compiler_params=pltpu.CompilerParams(
            collective_id=0, has_side_effects=True, vmem_limit_bytes=65000 * 1024
        ),
    )(
        tokens,
        norm_gain[None],
        *weights,
        map_lambda,
        diff_gain[None],
        decay_rate,
        state_gain[None],
        out_weight,
    )


def body(tokens, norm_gain, *rest):
    weights, (map_lambda, diff_gain, decay_rate, state_gain, out_weight) = rest[:6], rest[6:]
    line = lax.axis_size("sp")
    pair = lax.axis_size("tp")
    local = map_lambda.shape[0]
    if local != line or line < 3 or decay_rate.shape[0] != local or lax.axis_size("fs") != 4 or pair != 2:
        return spread_body(tokens, norm_gain, *rest)
    return whole_layer(
        tokens[0],
        norm_gain,
        weights,
        map_lambda,
        diff_gain,
        decay_rate,
        state_gain,
        out_weight,
        line,
        pair,
    )[None]


def solution(mesh):
    placed = (
        P("fs", "sp", "tp"),
        P(),
        P("fs", "tp"),
        P("fs", "tp"),
        P("fs", "tp"),
        P("fs", "tp"),
        P("fs", "tp"),
        P("fs", "tp"),
        P("tp"),
        P("tp"),
        P("tp"),
        P("tp"),
        P(),
    )
    return jax.shard_map(
        body, mesh=mesh, in_specs=placed, out_specs=P("fs", ("sp", "tp"), None), check_vma=False
    )
```

```python
import functools

import jax
import jax.numpy as jnp
from jax import lax
from jax.experimental import pallas as pl
from jax.experimental.pallas import tpu as pltpu
from jax.sharding import PartitionSpec as P

DK = 64
DV = 128
DR = 128


epsilon = 1e-05
branch_scale = 0.8
masked_score = -1e30


def from_behind(x, axis, by):
    size = lax.axis_size(axis)
    pairs = [(i, i + by) for i in range(size) if 0 <= i + by < size]
    return lax.ppermute(x, axis, pairs)


def entering(x, axis, join, neutral):
    place = lax.axis_index(axis)
    gathered = jax.tree.map(
        lambda a, kind: lax.all_gather(a.astype(kind), axis), x, (jnp.bfloat16, jnp.bfloat16)
    )
    state = jax.tree.map(lambda a, e: jnp.zeros_like(a) + jnp.asarray(e, a.dtype), x, neutral)

    def one(turn, state):
        return join(
            state,
            jax.tree.map(
                lambda a, own: lax.dynamic_index_in_dim(a, turn, 0, False).astype(own.dtype),
                gathered,
                x,
            ),
        )

    return lax.fori_loop(0, place, one, state)


def attend(att_query, att_keys, att_values, map_lambda, diff_gain):
    tok_rows = att_query.shape[0]
    head_count = map_lambda.shape[0]
    key_width = att_keys.shape[1]
    query_heads = att_query.reshape(tok_rows, head_count, 2, DK)
    sp_index = lax.axis_index("sp")
    query_place = sp_index * tok_rows + jnp.arange(tok_rows)
    score_scale = DK ** (-0.5)

    def absorb_block(running, inputs):
        key_block, key_place = inputs
        key_heads = key_block[:, :key_width].reshape(tok_rows, head_count, 2, DK)
        value_heads = key_block[:, key_width:].reshape(tok_rows, head_count, DV)
        scores = (
            jnp.einsum(
                "qhmd,khmd->mhqk", query_heads, key_heads, preferred_element_type=jnp.float32
            )
            * score_scale
        )
        causal = key_place[None, :] <= query_place[:, None]
        row_peak, totals, summed = running
        new_peak = jnp.maximum(row_peak, jnp.max(jnp.where(causal, scores, masked_score), axis=-1))
        weights = jnp.where(causal, jnp.exp(scores - new_peak[..., None]), 0.0)
        factor = jnp.exp(row_peak - new_peak)
        totals = totals * factor + jnp.sum(weights, axis=-1)
        summed = summed * factor[..., None] + jnp.einsum(
            "mhqk,khv->mhqv",
            weights.astype(jnp.bfloat16),
            value_heads,
            preferred_element_type=jnp.float32,
        )
        return ((new_peak, totals, summed), None)

    def absorb(running, pieces, first_row):
        piece_rows = pieces.shape[0]
        stacked = pieces.reshape(piece_rows // tok_rows, tok_rows, pieces.shape[1])
        places = (first_row + jnp.arange(piece_rows)).reshape(piece_rows // tok_rows, tok_rows)
        return lax.scan(absorb_block, running, (stacked, places))[0]

    starting = (
        jnp.full((2, head_count, tok_rows), masked_score, jnp.float32),
        jnp.zeros((2, head_count, tok_rows), jnp.float32),
        jnp.zeros((2, head_count, tok_rows, DV), jnp.float32),
    )
    joined_kv = jnp.concatenate([att_keys, att_values], axis=1)
    first_state = absorb(starting, joined_kv, sp_index * tok_rows)

    def relay_step(step_index, relay_state):
        running, moving = relay_state
        moving = from_behind(moving, "sp", 1)
        first_row = (sp_index - step_index) * tok_rows
        running = lax.cond(
            first_row >= 0,
            lambda holding: absorb(holding, moving, first_row),
            lambda holding: holding,
            running,
        )
        return (running, moving)

    running, _ = lax.fori_loop(1, lax.axis_size("sp"), relay_step, (first_state, joined_kv))
    row_peak, totals, summed = running
    averaged = summed / totals[..., None]
    differ = averaged[0] - map_lambda[:, None, None] * averaged[1]
    normed = differ * lax.rsqrt(jnp.mean(differ * differ, axis=-1, keepdims=True) + epsilon)
    normed = normed * diff_gain.reshape(head_count, 1, DV) * branch_scale
    return normed.transpose(1, 0, 2).reshape(tok_rows, head_count * DV).astype(jnp.bfloat16)


def retain(ret_query, ret_keys, ret_values, decay_rate, state_gain):
    tok_rows = ret_query.shape[0]
    head_count = decay_rate.shape[0]
    query_heads = ret_query.reshape(tok_rows, head_count, DR)
    key_heads = ret_keys.reshape(tok_rows, head_count, DR)
    value_heads = ret_values.reshape(tok_rows, head_count, DR)
    position = jnp.arange(tok_rows).astype(jnp.float32)
    distance = position[:, None] - position[None, :]
    decay_col = decay_rate[:, None, None]
    within = jnp.where(distance >= 0, jnp.exp(-decay_col * jnp.maximum(distance, 0.0)), 0.0)
    local_scores = (
        jnp.einsum("qhd,khd->hqk", query_heads, key_heads, preferred_element_type=jnp.float32)
        * within
    )
    intra_out = jnp.einsum(
        "hqk,khv->hqv",
        local_scores.astype(jnp.bfloat16),
        value_heads,
        preferred_element_type=jnp.float32,
    )
    key_decayed = key_heads.astype(jnp.float32) * jnp.exp(
        -decay_rate[None, :, None] * (tok_rows - 1.0 - position)[:, None, None]
    )
    own_state = jnp.einsum(
        "khd,khv->hdv",
        key_decayed,
        value_heads.astype(jnp.float32),
        precision=lax.Precision.HIGHEST,
    )
    block_decay = jnp.exp(-decay_rate * tok_rows)

    def link_states(earlier, later):
        return (earlier[0] * later[1][:, None, None] + later[0], earlier[1] * later[1])

    identity = (jnp.zeros_like(own_state), jnp.ones_like(block_decay))
    incoming, _ = entering((own_state, block_decay), "sp", link_states, identity)
    carried = jnp.einsum(
        "qhd,hdv->hqv", query_heads.astype(jnp.float32), incoming, precision=lax.Precision.HIGHEST
    )
    carried = carried * jnp.exp(-decay_col * (position + 1.0)[None, :, None])
    combined = intra_out + carried
    normed = combined * lax.rsqrt(jnp.mean(combined * combined, axis=-1, keepdims=True) + epsilon)
    normed = normed * state_gain.reshape(head_count, 1, DR)
    return normed.transpose(1, 0, 2).reshape(tok_rows, head_count * DR).astype(jnp.bfloat16)


def spread_body(
    tokens,
    norm_gain,
    query_weight,
    key_weight,
    value_weight,
    state_query,
    state_key,
    state_value,
    map_lambda,
    diff_gain,
    decay_rate,
    state_gain,
    out_weight,
):
    gathered = lax.all_gather(tokens[0], "tp", axis=1, tiled=True)
    tok_float = gathered.astype(jnp.float32)
    normed = tok_float * lax.rsqrt(
        jnp.mean(tok_float * tok_float, axis=-1, keepdims=True) + epsilon
    )
    normed = (normed * norm_gain).astype(jnp.bfloat16)
    pieces = (
        lax.all_gather(query_weight, "fs", axis=0, tiled=True),
        lax.all_gather(key_weight, "fs", axis=0, tiled=True),
        lax.all_gather(value_weight, "fs", axis=0, tiled=True),
        lax.all_gather(state_query, "fs", axis=0, tiled=True),
        lax.all_gather(state_key, "fs", axis=0, tiled=True),
        lax.all_gather(state_value, "fs", axis=0, tiled=True),
    )
    projected = tuple(
        (jnp.dot(normed, row_block, preferred_element_type=jnp.float32) for row_block in pieces)
    )
    att_query, att_keys, att_values, ret_query, ret_keys, ret_values = (
        member.astype(jnp.bfloat16) for member in projected
    )
    attended = attend(att_query, att_keys, att_values, map_lambda, diff_gain)
    retained = retain(ret_query, ret_keys, ret_values, decay_rate, state_gain)
    joined = jnp.concatenate([attended, retained], axis=1)
    diff_width = attended.shape[1]
    ret_width = retained.shape[1]
    tp_count = lax.axis_size("tp")
    tp_index = lax.axis_index("tp")
    own_rows = jnp.concatenate(
        [
            lax.dynamic_slice_in_dim(out_weight, tp_index * diff_width, diff_width, 0),
            lax.dynamic_slice_in_dim(
                out_weight, tp_count * diff_width + tp_index * ret_width, ret_width, 0
            ),
        ],
        axis=0,
    )
    output = lax.psum_scatter(
        jnp.dot(joined, own_rows, preferred_element_type=jnp.float32).astype(jnp.bfloat16),
        "tp",
        scatter_dimension=0,
        tiled=True,
    )
    return output[None]


def row_product(a, b):
    return lax.dot_general(a, b, (((1,), (1,)), ((), ())), preferred_element_type=jnp.float32)


MESH = pl.DeviceIdType.MESH


def greet(peers):
    barrier = pltpu.get_barrier_semaphore()
    count = 0
    for peer, present in peers:
        if present is None:
            pl.semaphore_signal(barrier, inc=1, device_id=peer, device_id_type=MESH)
            count = count + 1
        else:

            @pl.when(present)
            def _():
                pl.semaphore_signal(barrier, inc=1, device_id=peer, device_id_type=MESH)

            count = count + jnp.where(present, 1, 0)
    pl.semaphore_wait(barrier, count)


def layer_kernel(
    line,
    parts,
    tokens,
    gain_in,
    w0,
    w1,
    w2,
    w3,
    w4,
    w5,
    lam_in,
    dgain_in,
    rate_in,
    sgain_in,
    out_weight,
    result,
    gains,
    lam_ref,
    rate_ref,
    seq,
    normal,
    weight,
    proj,
    mine,
    joined,
    held,
    state,
    total,
    local_sem,
    held_sem,
    wsend,
    wrecv,
    lsend,
    lrecv,
    psend,
    precv,
    osend,
    orecv,
):
    f32, bf16 = jnp.float32, jnp.bfloat16
    weights = (w0, w1, w2, w3, w4, w5)
    kinds = len(weights)
    half_kinds = kinds // 2
    early_parts = parts // 2
    events = 2 * line - 1
    z, f, c = lax.axis_index("sp"), lax.axis_index("fs"), lax.axis_index("tp")
    block, half = tokens.shape
    piece = block // parts
    depth = w0.shape[0]
    width = weight.shape[1] // kinds
    rows_out = result.shape[0]
    model = seq.shape[1]
    me = c * line + z
    near = ({"fs": f ^ 1}, {"fs": f ^ 2})
    whose = (f ^ 1, f ^ 2, f ^ 3)
    def held_at(b, side, q):
        return seq.at[
            pl.ds(pl.multiple_of(b * block + q * piece, piece), piece),
            pl.ds(pl.multiple_of(side * half, half), half),
        ]

    def whole(b, side):
        return seq.at[
            pl.ds(pl.multiple_of(b * block, block), block),
            pl.ds(pl.multiple_of(side * half, half), half),
        ]

    def column(kind):
        return (2 * (kind % half_kinds) + kind // half_kinds) * width

    def stored(owner, kind):
        return weight.at[
            pl.ds(pl.multiple_of(owner * depth, depth), depth), column(kind) : column(kind) + width
        ]

    def slot(e):
        up = (e - 1) % 2 == 0
        s = (e - 1) // 2
        return z - 1 - s if up else z + 1 + s

    def along(e, b, q):
        target = z + 1 if (e - 1) % 2 == 0 else z - 1
        return pltpu.make_async_remote_copy(
            src_ref=held_at(b, c, q),
            dst_ref=held_at(b, c, q),
            send_sem=lsend.at[e],
            recv_sem=lrecv.at[e, q],
            device_id={"sp": jnp.clip(target, 0, line - 1)},
            device_id_type=MESH,
        ), (target >= 0) & (target < line)

    def across(e, b, side, q):
        return pltpu.make_async_remote_copy(
            src_ref=held_at(b, side, q),
            dst_ref=held_at(b, side, q),
            send_sem=psend.at[e],
            recv_sem=precv.at[e],
            device_id={"tp": 1 - c},
            device_id_type=MESH,
        )

    def all_along(e):
        return pltpu.make_async_remote_copy(
            src_ref=whole(z, c),
            dst_ref=whole(z, c),
            send_sem=lsend.at[e],
            recv_sem=lrecv.at[e, 0],
            device_id={"sp": z ^ 1},
            device_id_type=MESH,
        )

    def all_across(e, b):
        return pltpu.make_async_remote_copy(
            src_ref=whole(b, 1 - c),
            dst_ref=whole(b, 1 - c),
            send_sem=psend.at[e],
            recv_sem=precv.at[e],
            device_id={"tp": 1 - c},
            device_id_type=MESH,
        )

    def own_columns(kind):
        return weights[kind].at[:, pl.ds(pl.multiple_of(z * width, width), width)]

    def arrival(relation, kind):
        return kind if relation == kind // half_kinds else kinds + kind % half_kinds

    def spread(way, kind, source, owner, index):
        return pltpu.make_async_remote_copy(
            src_ref=source,
            dst_ref=stored(owner, kind),
            send_sem=wsend,
            recv_sem=wrecv.at[arrival(2 if index >= kinds else way, kind)],
            device_id=near[way],
            device_id_type=MESH,
        )

    def arrived(relation, kind):
        pltpu.make_async_remote_copy(
            src_ref=stored(whose[relation], kind),
            dst_ref=stored(whose[relation], kind),
            send_sem=wsend,
            recv_sem=wrecv.at[arrival(relation, kind)],
            device_id=near[0],
            device_id_type=MESH,
        ).wait_recv()

    def push(e, q, when=True):
        copy, present = along(e, z, q)

        @pl.when(present & when)
        def _():
            copy.start()

    def scatter(pair):
        for turn in range(2):
            for way in range(2):
                kind = pair + half_kinds * (turn ^ way)
                spread(way, kind, stored(f, kind), f, kind).start()

    first_copies = [pltpu.make_async_copy(tokens, whole(z, c), local_sem.at[0])]
    for kind in range(kinds):
        first_copies.append(
            pltpu.make_async_copy(own_columns(kind), stored(f, kind), local_sem.at[1])
        )
    for copy in first_copies:
        copy.start()
    greet(
        [
            (near[0], None),
            (near[1], None),
            ({"tp": 1 - c}, None),
            ({"sp": jnp.minimum(z + 1, line - 1)}, z + 1 < line),
            ({"sp": jnp.maximum(z - 1, 0)}, z > 0),
        ]
    )
    first_copies[0].wait()
    for q in range(parts):
        push(1, q, z >= 0 if q < early_parts else z == 0)
        push(2, q)
    own_rows = weight.at[pl.ds(pl.multiple_of(f * depth, depth), depth), :]
    pltpu.make_async_copy(own_rows, own_rows, local_sem.at[1]).wait()
    scatter(0)
    for q in range(parts):
        across(0, z, c, q).start()
    scatter(1)
    spots = ((gain_in, 0), (dgain_in, model), (sgain_in, model + dgain_in.shape[1]))
    for source, first in spots:
        pltpu.make_async_copy(
            source, gains.at[:, first : first + source.shape[1]], local_sem.at[2]
        ).start()
    rates = (
        pltpu.make_async_copy(lam_in, lam_ref, local_sem.at[3]),
        pltpu.make_async_copy(rate_in, rate_ref, local_sem.at[4]),
    )
    for copy in rates:
        copy.start()

    def relay(turn):
        for way in range(2):
            kind = turn + way * half_kinds
            arrived(way, kind)
            spread(1 - way, kind, stored(whose[way], kind), whose[way], kinds + turn).start()

    def complete(turn):
        landed = weight.at[: 2 * depth, 2 * turn * width : 2 * (turn + 1) * width]
        pltpu.make_async_remote_copy(
            src_ref=landed,
            dst_ref=landed,
            send_sem=wsend,
            recv_sem=wrecv.at[kinds + turn],
            device_id=near[0],
            device_id_type=MESH,
        ).wait_recv()

    def serve(e, q, when):
        b = slot(e)

        @pl.when((b >= 0) & (b < line) & when)
        def _():
            copy, _ = along(e, b, q)
            copy.wait_recv()
            if (e - 1) // 2 + 1 < line - 1:
                onward, present = along(e + 2, b, q)

                @pl.when(present)
                def _():
                    onward.start()

            across(e, b, c, q).start()

    def at_slot(k):
        for s in range(line - 1):
            for q in range(parts):
                if q < early_parts:
                    if k == s * early_parts + q:
                        serve(1 + 2 * s, q, z > s)
                else:
                    for other in range(s + 1, line):
                        if k == (2 * other - 4 - s) * early_parts + parts + q:
                            serve(1 + 2 * s, q, z == other)
        serve(2 + 2 * (k // parts), k % parts, z >= 0)
        if k % parts == parts - 1 and k // parts < line - 2:
            for q in range(early_parts, parts):
                push(1, q, z == k // parts + 1)

    def fetch(index):
        source = index // 2
        kind = index % 2
        first = kind * (out_weight.shape[0] // 2) + source * width
        return pltpu.make_async_copy(
            out_weight.at[first : first + width, :],
            held.at[source, kind * width : (kind + 1) * width, :],
            held_sem,
        )

    fetches = [fetch(index) for index in range(2 * joined.shape[0])]

    def block_of(e):
        s = (e - 1) // 2
        return jnp.where(e == 0, z, jnp.where((e - 1) % 2 == 0, z - 1 - s, z + 1 + s))

    def rows_of(b):
        return pl.ds(pl.multiple_of(b * block, block), block)

    def normalize(e, b):
        all_across(e, b).wait_recv()
        x = seq[rows_of(b), :].astype(f32)
        scaled = x * lax.rsqrt(jnp.mean(x * x, axis=1, keepdims=True) + epsilon)
        normal[rows_of(b), :] = (scaled * gains[:, :model]).astype(bf16)

    def project(b, first, count):
        columns = slice(2 * first * width, 2 * (first + count) * width)
        proj[rows_of(b), columns] = jnp.dot(
            normal[rows_of(b), :], weight[:, columns], preferred_element_type=f32
        ).astype(bf16)

    def soon(e, b):
        return (e == 0) | (((e == 2) | ((e == 1) & (z == 1))) & (b < line))

    def late(e):
        return ((z == line - 1) & (e % 2 == 1) & (e < events - 2)) | ((z == 0) & (e == events - 1))

    def normalize_some(first, last, chosen):
        def one(e, carry):
            b = block_of(e)

            @pl.when((b >= 0) & (b < line) & chosen(e, b))
            def _():
                normalize(e, b)

            return carry

        lax.fori_loop(first, last, one, 0)

    def project_ready(first, count):
        def one(b, carry):
            @pl.when(
                ((z > 0) | (b < line - 1)) & ((z < line - 1) | (b == 0) | (b == line - 1))
            )
            def _():
                project(b, first, count)

            return carry

        lax.fori_loop(0, line, one, 0)

    early_slots = parts * (line - 2)
    relay(0)
    scatter(2)
    for copy in fetches:
        copy.start()
    for k in range(early_slots):
        at_slot(k)
        if k < 2:
            relay(k + 1)
        if k == parts:
            for copy in rates:
                copy.wait()
            pltpu.make_async_copy(gains, gains, local_sem.at[2]).wait()
            normalize_some(0, 3, soon)
    normalize_some(1, events, lambda e, b: ~soon(e, b) & ~late(e))
    for turn in range(half_kinds - 1):
        complete(turn)
    project_ready(0, half_kinds - 1)
    complete(half_kinds - 1)
    project_ready(half_kinds - 1, 1)

    row = lax.broadcasted_iota(jnp.int32, (block, block), 0)
    col = lax.broadcasted_iota(jnp.int32, (block, block), 1)
    lane = lax.broadcasted_iota(jnp.int32, (block, 2 * DK), 1)
    position = lax.broadcasted_iota(jnp.int32, (block, 1), 0).astype(f32)

    def part(kind, first, count):
        return proj[first : first + count, column(kind) : column(kind) + DV]

    def mix(b):
        first = b * block
        causal = col <= row
        lam = lam_ref[z]
        rate = rate_ref[z]
        query = part(0, first, block) * jnp.asarray(DK ** (-0.5), bf16)
        averaged = []
        for which in range(2):
            own = jnp.where((lane >= DK) == bool(which), query, jnp.zeros_like(query))
            near_scores = jnp.where(causal, row_product(own, part(1, first, block)), masked_score)
            peak = jnp.max(near_scores, axis=1, keepdims=True)
            if first:
                far = row_product(own, part(1, 0, first))
                peak = jnp.maximum(peak, jnp.max(far, axis=1, keepdims=True))
            near_scores = jnp.exp(near_scores - peak)
            count = jnp.sum(near_scores, axis=1, keepdims=True)
            summed = jnp.dot(
                near_scores.astype(bf16), part(2, first, block), preferred_element_type=f32
            )
            if first:
                far = jnp.exp(far - peak)
                count = count + jnp.sum(far, axis=1, keepdims=True)
                summed = summed + jnp.dot(
                    far.astype(bf16), part(2, 0, first), preferred_element_type=f32
                )
            averaged.append(summed / count)
        differ = averaged[0] - lam * averaged[1]
        scaled = differ * lax.rsqrt(jnp.mean(differ * differ, axis=1, keepdims=True) + epsilon)
        mine[first : first + block, :DV] = (
            scaled * (gains[:, pl.ds(pl.multiple_of(model + z * DV, DV), DV)] * branch_scale)
        ).astype(bf16)
        ret_query = part(3, first, block)
        ret_keys = part(4, first, block)
        ret_values = part(5, first, block)
        within = jnp.where(causal, jnp.exp(-rate * jnp.maximum(row - col, 0).astype(f32)), 0.0)
        local = (row_product(ret_query, ret_keys) * within).astype(bf16)
        mixed = jnp.dot(local, ret_values, preferred_element_type=f32)
        if first:
            mixed = mixed + jnp.exp(-rate * (position + 1.0)) * jnp.dot(
                ret_query, state[...].astype(bf16), preferred_element_type=f32
            )
        if b + 1 < line:
            decayed = (ret_keys.astype(f32) * jnp.exp(-rate * (block - 1.0 - position))).astype(bf16)
            update = lax.dot_general(
                decayed, ret_values, (((0,), (0,)), ((), ())), preferred_element_type=f32
            )
            if first:
                update = state[...] * jnp.exp(jnp.full((1, DR), -block, f32) * rate) + update
            state[...] = update
        scaled = mixed * lax.rsqrt(jnp.mean(mixed * mixed, axis=1, keepdims=True) + epsilon)
        mine[first : first + block, DV:] = (scaled * gains[:, pl.ds(pl.multiple_of(model + dgain_in.shape[1] + z * DV, DV), DV)]).astype(bf16)

    def mine_rows(b, side):
        return mine.at[pl.ds(pl.multiple_of(b * block + side * rows_out, rows_out), rows_out), :]

    def deliver(b, h):
        return pltpu.make_async_remote_copy(
            src_ref=mine_rows(b, h),
            dst_ref=joined.at[me],
            send_sem=osend,
            recv_sem=orecv.at[me],
            device_id={"sp": b, "tp": h},
            device_id_type=MESH,
        )

    def own_place(b, h):
        return (z == b) & (c == h)

    def send(b, when):
        for h in range(2):

            @pl.when(when & ~own_place(b, h))
            def _():
                deliver(b, h).start()

    def give(b):
        if b == 0:
            send(b, z <= 1)
        elif b == line - 1:
            send(b, (z == 0) | (z >= line - 2))
        else:
            send(b, z >= 0)

        @pl.when(z == b)
        def _():
            joined[me] = mine_rows(b, c)[...]

    def last_token(end):
        if end == 0:
            return all_along(events - 1), z == 1
        return all_along(1), z == line - 2

    def phase(t, carry):
        @pl.when(t == line - 2)
        def _():
            for end in (0, line - 1):
                copy, here = last_token(end)

                @pl.when(here)
                def _():
                    copy.wait_send()

            send(0, z > 1)
            send(line - 1, (z > 0) & (z < line - 2))

        for turn in range(1, line - 1):

            @pl.when(t == turn)
            def _():
                for q in range(early_parts):
                    at_slot(early_slots + (turn - 1) * early_parts + q)

        @pl.when((t > 0) & ((z == line - 1) | ((z == 0) & (t == line - 2))))
        def _():
            b = jnp.where(z == 0, line - 1, t)
            e = jnp.where(z == 0, events - 1, 2 * (line - 2 - t) + 1)
            normalize(e, b)
            project(b, 0, half_kinds)

        for b in range(line):
            turn = jnp.where(z == line - 1, min(b, line - 2), 0)
            if b == line - 1:
                turn = jnp.where(z == 0, line - 2, turn)

            @pl.when(turn == t)
            def _():
                mix(b)
                give(b)

        return carry

    lax.fori_loop(0, line - 1, phase, 0)

    pltpu.make_async_copy(held, held, held_sem).wait()
    inner = [s for s in range(1, line - 1)]
    outer = (z == 0) | (z == line - 1)
    order = []
    for index in range(line):
        for_outer = ([0, line - 1] + inner)[index]
        for_inner = (inner + [0, line - 1])[index]
        order.append(jnp.where(outer, for_outer, for_inner))
    for index, source in enumerate(order):
        for turn in range(2):
            side = c if turn == 0 else 1 - c
            where = side * line + source

            @pl.when(where != me)
            def _():
                pltpu.make_async_remote_copy(
                    src_ref=joined.at[where],
                    dst_ref=joined.at[where],
                    send_sem=osend,
                    recv_sem=orecv.at[where],
                    device_id={"tp": 1 - c},
                    device_id_type=MESH,
                ).wait_recv()

            product = jnp.dot(joined[where], held[where], preferred_element_type=f32)
            if index == 0 and turn == 0:
                total[...] = product
            elif index < line - 1 or turn == 0:
                total[...] += product
            else:
                result[...] = (total[...] + product).astype(bf16)

    sent = weight.at[: 3 * depth, :]
    pltpu.make_async_remote_copy(
        src_ref=sent,
        dst_ref=sent,
        send_sem=wsend,
        recv_sem=wrecv.at[0],
        device_id=near[0],
        device_id_type=MESH,
    ).wait_send()
    for e in range(events):
        b = block_of(e)

        @pl.when((b >= 0) & (b < line))
        def _():
            all_across(e, b).wait_send()

        if e == 0:
            continue
        up = e % 2 == 1
        target = z + 1 if up else z - 1
        s = (e - 1) // 2
        source = z - s if up else z + s
        present = (target >= 0) & (target < line) & (source >= 0) & (source < line)
        if e == 1:
            present = present & (z != line - 2)
        if e == events - 1:
            present = present & (z != 1)

        @pl.when(present)
        def _():
            all_along(e).wait_send()

    gone = mine.at[: (2 * line - 1) * rows_out, :]
    pltpu.make_async_remote_copy(
        src_ref=gone,
        dst_ref=gone,
        send_sem=osend,
        recv_sem=orecv.at[0],
        device_id={"tp": 1 - c},
        device_id_type=MESH,
    ).wait_send()


def whole_layer(tokens, norm_gain, weights, map_lambda, diff_gain, decay_rate, state_gain, out_weight, line, pair):
    block, half = tokens.shape
    kinds = len(weights)
    model = norm_gain.shape[0]
    parts = 2
    rows = block // pair
    count = line * pair
    anywhere = pl.BlockSpec(memory_space=pl.ANY)
    vmem = pl.BlockSpec(memory_space=pltpu.VMEM)
    events = 2 * line - 1
    dma = pltpu.SemaphoreType.DMA
    bf16 = jnp.bfloat16
    operands = (
        tokens,
        norm_gain[None],
        *weights,
        map_lambda,
        diff_gain[None],
        decay_rate,
        state_gain[None],
        out_weight,
    )
    return pl.pallas_call(
        functools.partial(layer_kernel, line, parts),
        out_shape=jax.ShapeDtypeStruct((rows, out_weight.shape[1]), bf16),
        in_specs=[anywhere] * (kinds + 7),
        out_specs=vmem,
        scratch_shapes=[
            pltpu.VMEM((1, model + diff_gain.shape[0] + state_gain.shape[0]), jnp.float32),
            pltpu.SMEM(map_lambda.shape, jnp.float32),
            pltpu.SMEM(decay_rate.shape, jnp.float32),
            pltpu.VMEM((line * block, model), bf16),
            pltpu.VMEM((line * block, model), bf16),
            pltpu.VMEM((model, kinds * DV), bf16),
            pltpu.VMEM((line * block, kinds * DV), bf16),
            pltpu.VMEM((line * block, 2 * DV), bf16),
            pltpu.VMEM((count, rows, 2 * DV), bf16),
            pltpu.VMEM((count, 2 * DV, out_weight.shape[1]), bf16),
            pltpu.VMEM((DR, DR), jnp.float32),
            pltpu.VMEM((rows, out_weight.shape[1]), jnp.float32),
            dma((5,)),
            dma,
            dma,
            dma((kinds + kinds // 2,)),
            dma((events,)),
            dma((events, parts)),
            dma((events,)),
            dma((events,)),
            dma,
            dma((count,)),
        ],
        compiler_params=pltpu.CompilerParams(
            collective_id=0, has_side_effects=True, vmem_limit_bytes=40000 * 1024
        ),
    )(
        *(pltpu.with_memory_space_constraint(a, pltpu.HBM) for a in operands)
    )


def body(tokens, norm_gain, *rest):
    weights, (map_lambda, diff_gain, decay_rate, state_gain, out_weight) = rest[:6], rest[6:]
    line = lax.axis_size("sp")
    pair = lax.axis_size("tp")
    local = map_lambda.shape[0]
    if local != line or line < 3 or decay_rate.shape[0] != local or lax.axis_size("fs") != 4 or pair != 2:
        return spread_body(tokens, norm_gain, *rest)
    return whole_layer(
        tokens[0],
        norm_gain,
        weights,
        map_lambda,
        diff_gain,
        decay_rate,
        state_gain,
        out_weight,
        line,
        pair,
    )[None]


def solution(mesh):
    placed = (
        P("fs", "sp", "tp"),
        P(),
        P("fs", "tp"),
        P("fs", "tp"),
        P("fs", "tp"),
        P("fs", "tp"),
        P("fs", "tp"),
        P("fs", "tp"),
        P("tp"),
        P("tp"),
        P("tp"),
        P("tp"),
        P(),
    )
    return jax.shard_map(
        body, mesh=mesh, in_specs=placed, out_specs=P("fs", ("sp", "tp"), None), check_vma=False
    )
```

```python
import functools

import jax
import jax.numpy as jnp
from jax import lax
from jax.experimental import pallas as pl
from jax.experimental.pallas import tpu as pltpu
from jax.sharding import PartitionSpec as P

DK = 64
DV = 128
DR = 128


epsilon = 1e-05
branch_scale = 0.8
masked_score = -1e30


def from_behind(x, axis, by):
    size = lax.axis_size(axis)
    pairs = [(i, i + by) for i in range(size) if 0 <= i + by < size]
    return lax.ppermute(x, axis, pairs)


def entering(x, axis, join, neutral):
    place = lax.axis_index(axis)
    gathered = jax.tree.map(
        lambda a, kind: lax.all_gather(a.astype(kind), axis), x, (jnp.bfloat16, jnp.bfloat16)
    )
    state = jax.tree.map(lambda a, e: jnp.zeros_like(a) + jnp.asarray(e, a.dtype), x, neutral)

    def one(turn, state):
        return join(
            state,
            jax.tree.map(
                lambda a, own: lax.dynamic_index_in_dim(a, turn, 0, False).astype(own.dtype),
                gathered,
                x,
            ),
        )

    return lax.fori_loop(0, place, one, state)


def attend(att_query, att_keys, att_values, map_lambda, diff_gain):
    tok_rows = att_query.shape[0]
    head_count = map_lambda.shape[0]
    key_width = att_keys.shape[1]
    query_heads = att_query.reshape(tok_rows, head_count, 2, DK)
    sp_index = lax.axis_index("sp")
    query_place = sp_index * tok_rows + jnp.arange(tok_rows)
    score_scale = DK ** (-0.5)

    def absorb_block(running, inputs):
        key_block, key_place = inputs
        key_heads = key_block[:, :key_width].reshape(tok_rows, head_count, 2, DK)
        value_heads = key_block[:, key_width:].reshape(tok_rows, head_count, DV)
        scores = (
            jnp.einsum(
                "qhmd,khmd->mhqk", query_heads, key_heads, preferred_element_type=jnp.float32
            )
            * score_scale
        )
        causal = key_place[None, :] <= query_place[:, None]
        row_peak, totals, summed = running
        new_peak = jnp.maximum(row_peak, jnp.max(jnp.where(causal, scores, masked_score), axis=-1))
        weights = jnp.where(causal, jnp.exp(scores - new_peak[..., None]), 0.0)
        factor = jnp.exp(row_peak - new_peak)
        totals = totals * factor + jnp.sum(weights, axis=-1)
        summed = summed * factor[..., None] + jnp.einsum(
            "mhqk,khv->mhqv",
            weights.astype(jnp.bfloat16),
            value_heads,
            preferred_element_type=jnp.float32,
        )
        return ((new_peak, totals, summed), None)

    def absorb(running, pieces, first_row):
        piece_rows = pieces.shape[0]
        stacked = pieces.reshape(piece_rows // tok_rows, tok_rows, pieces.shape[1])
        places = (first_row + jnp.arange(piece_rows)).reshape(piece_rows // tok_rows, tok_rows)
        return lax.scan(absorb_block, running, (stacked, places))[0]

    starting = (
        jnp.full((2, head_count, tok_rows), masked_score, jnp.float32),
        jnp.zeros((2, head_count, tok_rows), jnp.float32),
        jnp.zeros((2, head_count, tok_rows, DV), jnp.float32),
    )
    joined_kv = jnp.concatenate([att_keys, att_values], axis=1)
    first_state = absorb(starting, joined_kv, sp_index * tok_rows)

    def relay_step(step_index, relay_state):
        running, moving = relay_state
        moving = from_behind(moving, "sp", 1)
        first_row = (sp_index - step_index) * tok_rows
        running = lax.cond(
            first_row >= 0,
            lambda holding: absorb(holding, moving, first_row),
            lambda holding: holding,
            running,
        )
        return (running, moving)

    running, _ = lax.fori_loop(1, lax.axis_size("sp"), relay_step, (first_state, joined_kv))
    row_peak, totals, summed = running
    averaged = summed / totals[..., None]
    differ = averaged[0] - map_lambda[:, None, None] * averaged[1]
    normed = differ * lax.rsqrt(jnp.mean(differ * differ, axis=-1, keepdims=True) + epsilon)
    normed = normed * diff_gain.reshape(head_count, 1, DV) * branch_scale
    return normed.transpose(1, 0, 2).reshape(tok_rows, head_count * DV).astype(jnp.bfloat16)


def retain(ret_query, ret_keys, ret_values, decay_rate, state_gain):
    tok_rows = ret_query.shape[0]
    head_count = decay_rate.shape[0]
    query_heads = ret_query.reshape(tok_rows, head_count, DR)
    key_heads = ret_keys.reshape(tok_rows, head_count, DR)
    value_heads = ret_values.reshape(tok_rows, head_count, DR)
    position = jnp.arange(tok_rows).astype(jnp.float32)
    distance = position[:, None] - position[None, :]
    decay_col = decay_rate[:, None, None]
    within = jnp.where(distance >= 0, jnp.exp(-decay_col * jnp.maximum(distance, 0.0)), 0.0)
    local_scores = (
        jnp.einsum("qhd,khd->hqk", query_heads, key_heads, preferred_element_type=jnp.float32)
        * within
    )
    intra_out = jnp.einsum(
        "hqk,khv->hqv",
        local_scores.astype(jnp.bfloat16),
        value_heads,
        preferred_element_type=jnp.float32,
    )
    key_decayed = key_heads.astype(jnp.float32) * jnp.exp(
        -decay_rate[None, :, None] * (tok_rows - 1.0 - position)[:, None, None]
    )
    own_state = jnp.einsum(
        "khd,khv->hdv",
        key_decayed,
        value_heads.astype(jnp.float32),
        precision=lax.Precision.HIGHEST,
    )
    block_decay = jnp.exp(-decay_rate * tok_rows)

    def link_states(earlier, later):
        return (earlier[0] * later[1][:, None, None] + later[0], earlier[1] * later[1])

    identity = (jnp.zeros_like(own_state), jnp.ones_like(block_decay))
    incoming, _ = entering((own_state, block_decay), "sp", link_states, identity)
    carried = jnp.einsum(
        "qhd,hdv->hqv", query_heads.astype(jnp.float32), incoming, precision=lax.Precision.HIGHEST
    )
    carried = carried * jnp.exp(-decay_col * (position + 1.0)[None, :, None])
    combined = intra_out + carried
    normed = combined * lax.rsqrt(jnp.mean(combined * combined, axis=-1, keepdims=True) + epsilon)
    normed = normed * state_gain.reshape(head_count, 1, DR)
    return normed.transpose(1, 0, 2).reshape(tok_rows, head_count * DR).astype(jnp.bfloat16)


def spread_body(
    tokens,
    norm_gain,
    query_weight,
    key_weight,
    value_weight,
    state_query,
    state_key,
    state_value,
    map_lambda,
    diff_gain,
    decay_rate,
    state_gain,
    out_weight,
):
    gathered = lax.all_gather(tokens[0], "tp", axis=1, tiled=True)
    tok_float = gathered.astype(jnp.float32)
    normed = tok_float * lax.rsqrt(
        jnp.mean(tok_float * tok_float, axis=-1, keepdims=True) + epsilon
    )
    normed = (normed * norm_gain).astype(jnp.bfloat16)
    pieces = (
        lax.all_gather(query_weight, "fs", axis=0, tiled=True),
        lax.all_gather(key_weight, "fs", axis=0, tiled=True),
        lax.all_gather(value_weight, "fs", axis=0, tiled=True),
        lax.all_gather(state_query, "fs", axis=0, tiled=True),
        lax.all_gather(state_key, "fs", axis=0, tiled=True),
        lax.all_gather(state_value, "fs", axis=0, tiled=True),
    )
    projected = tuple(
        (jnp.dot(normed, row_block, preferred_element_type=jnp.float32) for row_block in pieces)
    )
    att_query, att_keys, att_values, ret_query, ret_keys, ret_values = (
        member.astype(jnp.bfloat16) for member in projected
    )
    attended = attend(att_query, att_keys, att_values, map_lambda, diff_gain)
    retained = retain(ret_query, ret_keys, ret_values, decay_rate, state_gain)
    joined = jnp.concatenate([attended, retained], axis=1)
    diff_width = attended.shape[1]
    ret_width = retained.shape[1]
    tp_count = lax.axis_size("tp")
    tp_index = lax.axis_index("tp")
    own_rows = jnp.concatenate(
        [
            lax.dynamic_slice_in_dim(out_weight, tp_index * diff_width, diff_width, 0),
            lax.dynamic_slice_in_dim(
                out_weight, tp_count * diff_width + tp_index * ret_width, ret_width, 0
            ),
        ],
        axis=0,
    )
    output = lax.psum_scatter(
        jnp.dot(joined, own_rows, preferred_element_type=jnp.float32).astype(jnp.bfloat16),
        "tp",
        scatter_dimension=0,
        tiled=True,
    )
    return output[None]


def row_product(a, b):
    return lax.dot_general(a, b, (((1,), (1,)), ((), ())), preferred_element_type=jnp.float32)


MESH = pl.DeviceIdType.MESH


def greet(peers):
    barrier = pltpu.get_barrier_semaphore()
    count = 0
    for peer, present in peers:
        if present is None:
            pl.semaphore_signal(barrier, inc=1, device_id=peer, device_id_type=MESH)
            count = count + 1
        else:

            @pl.when(present)
            def _():
                pl.semaphore_signal(barrier, inc=1, device_id=peer, device_id_type=MESH)

            count = count + jnp.where(present, 1, 0)
    pl.semaphore_wait(barrier, count)


def layer_kernel(
    line,
    parts,
    tokens,
    gain_in,
    w0,
    w1,
    w2,
    w3,
    w4,
    w5,
    lam_in,
    dgain_in,
    rate_in,
    sgain_in,
    out_weight,
    result,
    gains,
    lam_ref,
    rate_ref,
    seq,
    normal,
    weight,
    proj,
    mine,
    joined,
    held,
    state,
    total,
    local_sem,
    held_sem,
    wsend,
    wrecv,
    lsend,
    lrecv,
    psend,
    precv,
    osend,
    orecv,
):
    f32, bf16 = jnp.float32, jnp.bfloat16
    weights = (w0, w1, w2, w3, w4, w5)
    kinds = len(weights)
    half_kinds = kinds // 2
    early_parts = parts // 2
    events = 2 * line - 1
    z, f, c = lax.axis_index("sp"), lax.axis_index("fs"), lax.axis_index("tp")
    block, half = tokens.shape
    piece = block // parts
    depth = w0.shape[0]
    width = weight.shape[1] // kinds
    rows_out = result.shape[0]
    model = seq.shape[1]
    me = c * line + z
    near = ({"fs": f ^ 1}, {"fs": f ^ 2})
    whose = (f ^ 1, f ^ 2, f ^ 3)
    def held_at(b, side, q):
        return seq.at[
            pl.ds(pl.multiple_of(b * block + q * piece, piece), piece),
            pl.ds(pl.multiple_of(side * half, half), half),
        ]

    def whole(b, side):
        return seq.at[
            pl.ds(pl.multiple_of(b * block, block), block),
            pl.ds(pl.multiple_of(side * half, half), half),
        ]

    def column(kind):
        return (2 * (kind % half_kinds) + kind // half_kinds) * width

    def stored(owner, kind):
        return weight.at[
            pl.ds(pl.multiple_of(owner * depth, depth), depth), column(kind) : column(kind) + width
        ]

    def slot(e):
        up = (e - 1) % 2 == 0
        s = (e - 1) // 2
        return z - 1 - s if up else z + 1 + s

    def along(e, b, q):
        target = z + 1 if (e - 1) % 2 == 0 else z - 1
        return pltpu.make_async_remote_copy(
            src_ref=held_at(b, c, q),
            dst_ref=held_at(b, c, q),
            send_sem=lsend.at[e],
            recv_sem=lrecv.at[e, q],
            device_id={"sp": jnp.clip(target, 0, line - 1)},
            device_id_type=MESH,
        ), (target >= 0) & (target < line)

    def across(e, b, side, q):
        return pltpu.make_async_remote_copy(
            src_ref=held_at(b, side, q),
            dst_ref=held_at(b, side, q),
            send_sem=psend.at[e],
            recv_sem=precv.at[e, q],
            device_id={"tp": 1 - c},
            device_id_type=MESH,
        )

    def all_along(e):
        return pltpu.make_async_remote_copy(
            src_ref=whole(z, c),
            dst_ref=whole(z, c),
            send_sem=lsend.at[e],
            recv_sem=lrecv.at[e, 0],
            device_id={"sp": z ^ 1},
            device_id_type=MESH,
        )

    def all_across(e, b):
        return pltpu.make_async_remote_copy(
            src_ref=whole(b, 1 - c),
            dst_ref=whole(b, 1 - c),
            send_sem=psend.at[e],
            recv_sem=precv.at[e, 0],
            device_id={"tp": 1 - c},
            device_id_type=MESH,
        )

    def own_columns(kind):
        return weights[kind].at[:, pl.ds(pl.multiple_of(z * width, width), width)]

    def arrival(relation, kind):
        return kind if relation == kind // half_kinds else kinds + kind % half_kinds

    def spread(way, kind, source, owner, index):
        return pltpu.make_async_remote_copy(
            src_ref=source,
            dst_ref=stored(owner, kind),
            send_sem=wsend,
            recv_sem=wrecv.at[arrival(2 if index >= kinds else way, kind)],
            device_id=near[way],
            device_id_type=MESH,
        )

    def arrived(relation, kind):
        pltpu.make_async_remote_copy(
            src_ref=stored(whose[relation], kind),
            dst_ref=stored(whose[relation], kind),
            send_sem=wsend,
            recv_sem=wrecv.at[arrival(relation, kind)],
            device_id=near[0],
            device_id_type=MESH,
        ).wait_recv()

    def push(e, q, when=True):
        copy, present = along(e, z, q)

        @pl.when(present & when)
        def _():
            copy.start()

    def scatter(pair):
        for turn in range(2):
            for way in range(2):
                kind = pair + half_kinds * (turn ^ way)
                spread(way, kind, stored(f, kind), f, kind).start()

    first_copies = [pltpu.make_async_copy(tokens, whole(z, c), local_sem.at[0])]
    for kind in range(kinds):
        first_copies.append(
            pltpu.make_async_copy(own_columns(kind), stored(f, kind), local_sem.at[1])
        )
    for copy in first_copies:
        copy.start()
    greet(
        [
            (near[0], None),
            (near[1], None),
            ({"tp": 1 - c}, None),
            ({"sp": jnp.minimum(z + 1, line - 1)}, z + 1 < line),
            ({"sp": jnp.maximum(z - 1, 0)}, z > 0),
        ]
    )
    first_copies[0].wait()
    for q in range(parts):
        push(1, q, z >= 0 if q < early_parts else z == 0)
        push(2, q)
    own_rows = weight.at[pl.ds(pl.multiple_of(f * depth, depth), depth), :]
    pltpu.make_async_copy(own_rows, own_rows, local_sem.at[1]).wait()
    scatter(0)
    for q in range(parts):
        across(0, z, c, q).start()
    scatter(1)
    spots = ((gain_in, 0), (dgain_in, model), (sgain_in, model + dgain_in.shape[1]))
    for source, first in spots:
        pltpu.make_async_copy(
            source, gains.at[:, first : first + source.shape[1]], local_sem.at[2]
        ).start()
    rates = (
        pltpu.make_async_copy(lam_in, lam_ref, local_sem.at[3]),
        pltpu.make_async_copy(rate_in, rate_ref, local_sem.at[4]),
    )
    for copy in rates:
        copy.start()

    def relay(turn):
        for way in range(2):
            kind = turn + way * half_kinds
            arrived(way, kind)
            spread(1 - way, kind, stored(whose[way], kind), whose[way], kinds + turn).start()

    def complete(turn):
        landed = weight.at[: 2 * depth, 2 * turn * width : 2 * (turn + 1) * width]
        pltpu.make_async_remote_copy(
            src_ref=landed,
            dst_ref=landed,
            send_sem=wsend,
            recv_sem=wrecv.at[kinds + turn],
            device_id=near[0],
            device_id_type=MESH,
        ).wait_recv()

    def serve(e, q, when):
        b = slot(e)

        @pl.when((b >= 0) & (b < line) & when)
        def _():
            copy, _ = along(e, b, q)
            copy.wait_recv()
            if (e - 1) // 2 + 1 < line - 1:
                onward, present = along(e + 2, b, q)

                @pl.when(present)
                def _():
                    onward.start()

            across(e, b, c, q).start()

    def at_slot(k):
        for s in range(line - 1):
            for q in range(parts):
                if q < early_parts:
                    if k == s * early_parts + q:
                        serve(1 + 2 * s, q, z > s)
                else:
                    for other in range(s + 1, line):
                        if k == (2 * other - 4 - s) * early_parts + parts + q:
                            serve(1 + 2 * s, q, z == other)
        serve(2 + 2 * (k // parts), k % parts, z >= 0)
        if k % parts == parts - 1 and k // parts < line - 2:
            for q in range(early_parts, parts):
                push(1, q, z == k // parts + 1)

    def fetch(index):
        source = index // 2
        kind = index % 2
        first = kind * (out_weight.shape[0] // 2) + source * width
        return pltpu.make_async_copy(
            out_weight.at[first : first + width, :],
            held.at[source, kind * width : (kind + 1) * width, :],
            held_sem,
        )

    fetches = [fetch(index) for index in range(2 * joined.shape[0])]

    def block_of(e):
        s = (e - 1) // 2
        return jnp.where(e == 0, z, jnp.where((e - 1) % 2 == 0, z - 1 - s, z + 1 + s))

    def rows_of(b):
        return pl.ds(pl.multiple_of(b * block, block), block)

    def normalize(e, b):
        for q in range(parts):
            across(e, b, 1 - c, q).wait_recv()
        x = seq[rows_of(b), :].astype(f32)
        scaled = x * lax.rsqrt(jnp.mean(x * x, axis=1, keepdims=True) + epsilon)
        normal[rows_of(b), :] = (scaled * gains[:, :model]).astype(bf16)

    def project(b, first, count):
        columns = slice(2 * first * width, 2 * (first + count) * width)
        proj[rows_of(b), columns] = jnp.dot(
            normal[rows_of(b), :], weight[:, columns], preferred_element_type=f32
        ).astype(bf16)

    def soon(e, b):
        return (e == 0) | (((e == 2) | ((e == 1) & (z == 1))) & (b < line))

    def late(e):
        return ((z == line - 1) & (e % 2 == 1) & (e < events - 2)) | ((z == 0) & (e == events - 1))

    def normalize_some(first, last, chosen):
        def one(e, carry):
            b = block_of(e)

            @pl.when((b >= 0) & (b < line) & chosen(e, b))
            def _():
                normalize(e, b)

            return carry

        lax.fori_loop(first, last, one, 0)

    def project_ready(first, count):
        def one(b, carry):
            @pl.when(
                ((z > 0) | (b < line - 1)) & ((z < line - 1) | (b == 0) | (b == line - 1))
            )
            def _():
                project(b, first, count)

            return carry

        lax.fori_loop(0, line, one, 0)

    early_slots = parts * (line - 2)
    relay(0)
    scatter(2)
    for copy in fetches:
        copy.start()
    for k in range(early_slots):
        at_slot(k)
        if k < 2:
            relay(k + 1)
        if k == parts:
            for copy in rates:
                copy.wait()
            pltpu.make_async_copy(gains, gains, local_sem.at[2]).wait()
            normalize_some(0, 3, soon)
    normalize_some(1, events, lambda e, b: ~soon(e, b) & ~late(e))
    for turn in range(half_kinds - 1):
        complete(turn)
    project_ready(0, half_kinds - 1)
    complete(half_kinds - 1)
    project_ready(half_kinds - 1, 1)

    row = lax.broadcasted_iota(jnp.int32, (block, block), 0)
    col = lax.broadcasted_iota(jnp.int32, (block, block), 1)
    lane = lax.broadcasted_iota(jnp.int32, (block, 2 * DK), 1)
    position = lax.broadcasted_iota(jnp.int32, (block, 1), 0).astype(f32)

    def part(kind, first, count):
        return proj[first : first + count, column(kind) : column(kind) + DV]

    def mix(b):
        first = b * block
        causal = col <= row
        lam = lam_ref[z]
        rate = rate_ref[z]
        query = part(0, first, block) * jnp.asarray(DK ** (-0.5), bf16)
        averaged = []
        for which in range(2):
            own = jnp.where((lane >= DK) == bool(which), query, jnp.zeros_like(query))
            near_scores = jnp.where(causal, row_product(own, part(1, first, block)), masked_score)
            peak = jnp.max(near_scores, axis=1, keepdims=True)
            if first:
                far = row_product(own, part(1, 0, first))
                peak = jnp.maximum(peak, jnp.max(far, axis=1, keepdims=True))
            near_scores = jnp.exp(near_scores - peak)
            count = jnp.sum(near_scores, axis=1, keepdims=True)
            summed = jnp.dot(
                near_scores.astype(bf16), part(2, first, block), preferred_element_type=f32
            )
            if first:
                far = jnp.exp(far - peak)
                count = count + jnp.sum(far, axis=1, keepdims=True)
                summed = summed + jnp.dot(
                    far.astype(bf16), part(2, 0, first), preferred_element_type=f32
                )
            averaged.append(summed / count)
        differ = averaged[0] - lam * averaged[1]
        scaled = differ * lax.rsqrt(jnp.mean(differ * differ, axis=1, keepdims=True) + epsilon)
        mine[first : first + block, :DV] = (
            scaled * (gains[:, pl.ds(pl.multiple_of(model + z * DV, DV), DV)] * branch_scale)
        ).astype(bf16)
        ret_query = part(3, first, block)
        ret_keys = part(4, first, block)
        ret_values = part(5, first, block)
        within = jnp.where(causal, jnp.exp(-rate * jnp.maximum(row - col, 0).astype(f32)), 0.0)
        local = (row_product(ret_query, ret_keys) * within).astype(bf16)
        mixed = jnp.dot(local, ret_values, preferred_element_type=f32)
        if first:
            mixed = mixed + jnp.exp(-rate * (position + 1.0)) * jnp.dot(
                ret_query, state[...].astype(bf16), preferred_element_type=f32
            )
        if b + 1 < line:
            decayed = (ret_keys.astype(f32) * jnp.exp(-rate * (block - 1.0 - position))).astype(bf16)
            update = lax.dot_general(
                decayed, ret_values, (((0,), (0,)), ((), ())), preferred_element_type=f32
            )
            if first:
                update = state[...] * jnp.exp(jnp.full((1, DR), -block, f32) * rate) + update
            state[...] = update
        scaled = mixed * lax.rsqrt(jnp.mean(mixed * mixed, axis=1, keepdims=True) + epsilon)
        mine[first : first + block, DV:] = (scaled * gains[:, pl.ds(pl.multiple_of(model + dgain_in.shape[1] + z * DV, DV), DV)]).astype(bf16)

    def mine_rows(b, side):
        return mine.at[pl.ds(pl.multiple_of(b * block + side * rows_out, rows_out), rows_out), :]

    def deliver(b, h):
        return pltpu.make_async_remote_copy(
            src_ref=mine_rows(b, h),
            dst_ref=joined.at[me],
            send_sem=osend,
            recv_sem=orecv.at[me],
            device_id={"sp": b, "tp": h},
            device_id_type=MESH,
        )

    def own_place(b, h):
        return (z == b) & (c == h)

    def send(b, when, halves=(0, 1)):
        for h in halves:

            @pl.when(when & ~own_place(b, h))
            def _():
                deliver(b, h).start()

    def give(b):
        if b == 0:
            send(b, z <= 1)
        elif b == line - 1:
            send(b, (z == 0) | (z >= line - 2))
        else:
            send(b, z >= 0)

        @pl.when(z == b)
        def _():
            joined[me] = mine_rows(b, c)[...]

    def last_token(end):
        if end == 0:
            return all_along(events - 1), z == 1
        return all_along(1), z == line - 2

    def phase(t, carry):
        @pl.when(t == line - 2)
        def _():
            for end in (0, line - 1):
                copy, here = last_token(end)

                @pl.when(here)
                def _():
                    copy.wait_send()

            send(0, (z > 1) & (z < line - 1))
            send(0, z == line - 1, (1,))
            send(line - 1, (z > 0) & (z < line - 2))

        @pl.when(t == line - 3)
        def _():
            send(0, z == line - 1, (0,))

        for turn in range(1, line - 1):

            @pl.when(t == turn)
            def _():
                for q in range(early_parts):
                    at_slot(early_slots + (turn - 1) * early_parts + q)

        @pl.when((t > 0) & ((z == line - 1) | ((z == 0) & (t <= parts))))
        def _():
            b = jnp.where(z == 0, line - 1, t)
            e = jnp.where(z == 0, events - 1, 2 * (line - 2 - t) + 1)

            def one(q, carry):
                across(e, b, 1 - c, q).wait_recv()
                rows = pl.ds(pl.multiple_of(b * block + q * piece, piece), piece)
                x = seq[rows, :].astype(f32)
                scaled = x * lax.rsqrt(jnp.mean(x * x, axis=1, keepdims=True) + epsilon)
                normal[rows, :] = (scaled * gains[:, :model]).astype(bf16)
                proj[rows, :] = jnp.dot(
                    normal[rows, :], weight[...], preferred_element_type=f32
                ).astype(bf16)
                return carry

            lax.fori_loop(
                jnp.where(z == 0, t - 1, 0), jnp.where(z == 0, t, parts), one, 0
            )

        for b in range(line):
            turn = jnp.where(z == line - 1, min(b, line - 2), 0)
            if b == line - 1:
                turn = jnp.where(z == 0, line - 2, turn)

            @pl.when(turn == t)
            def _():
                mix(b)
                give(b)

        return carry

    lax.fori_loop(0, line - 1, phase, 0)

    pltpu.make_async_copy(held, held, held_sem).wait()
    inner = [s for s in range(1, line - 1)]
    outer = (z == 0) | (z == line - 1)
    order = []
    for index in range(line):
        for_outer = ([0, line - 1] + inner)[index]
        for_inner = (inner + [0, line - 1])[index]
        order.append(jnp.where(outer, for_outer, for_inner))
    for index, source in enumerate(order):
        for turn in range(2):
            side = c if turn == 0 else 1 - c
            where = side * line + source

            @pl.when(where != me)
            def _():
                pltpu.make_async_remote_copy(
                    src_ref=joined.at[where],
                    dst_ref=joined.at[where],
                    send_sem=osend,
                    recv_sem=orecv.at[where],
                    device_id={"tp": 1 - c},
                    device_id_type=MESH,
                ).wait_recv()

            product = jnp.dot(joined[where], held[where], preferred_element_type=f32)
            if index == 0 and turn == 0:
                total[...] = product
            elif index < line - 1 or turn == 0:
                total[...] += product
            else:
                result[...] = (total[...] + product).astype(bf16)

    sent = weight.at[: 3 * depth, :]
    pltpu.make_async_remote_copy(
        src_ref=sent,
        dst_ref=sent,
        send_sem=wsend,
        recv_sem=wrecv.at[0],
        device_id=near[0],
        device_id_type=MESH,
    ).wait_send()
    for e in range(events):
        b = block_of(e)

        @pl.when((b >= 0) & (b < line))
        def _():
            all_across(e, b).wait_send()

        if e == 0:
            continue
        up = e % 2 == 1
        target = z + 1 if up else z - 1
        s = (e - 1) // 2
        source = z - s if up else z + s
        present = (target >= 0) & (target < line) & (source >= 0) & (source < line)
        if e == 1:
            present = present & (z != line - 2)
        if e == events - 1:
            present = present & (z != 1)

        @pl.when(present)
        def _():
            all_along(e).wait_send()

    gone = mine.at[: (2 * line - 1) * rows_out, :]
    pltpu.make_async_remote_copy(
        src_ref=gone,
        dst_ref=gone,
        send_sem=osend,
        recv_sem=orecv.at[0],
        device_id={"tp": 1 - c},
        device_id_type=MESH,
    ).wait_send()


def whole_layer(tokens, norm_gain, weights, map_lambda, diff_gain, decay_rate, state_gain, out_weight, line, pair):
    block, half = tokens.shape
    kinds = len(weights)
    model = norm_gain.shape[0]
    parts = 2
    rows = block // pair
    count = line * pair
    anywhere = pl.BlockSpec(memory_space=pl.ANY)
    vmem = pl.BlockSpec(memory_space=pltpu.VMEM)
    events = 2 * line - 1
    dma = pltpu.SemaphoreType.DMA
    bf16 = jnp.bfloat16
    operands = (
        tokens,
        norm_gain[None],
        *weights,
        map_lambda,
        diff_gain[None],
        decay_rate,
        state_gain[None],
        out_weight,
    )
    return pl.pallas_call(
        functools.partial(layer_kernel, line, parts),
        out_shape=jax.ShapeDtypeStruct((rows, out_weight.shape[1]), bf16),
        in_specs=[anywhere] * (kinds + 7),
        out_specs=vmem,
        scratch_shapes=[
            pltpu.VMEM((1, model + diff_gain.shape[0] + state_gain.shape[0]), jnp.float32),
            pltpu.SMEM(map_lambda.shape, jnp.float32),
            pltpu.SMEM(decay_rate.shape, jnp.float32),
            pltpu.VMEM((line * block, model), bf16),
            pltpu.VMEM((line * block, model), bf16),
            pltpu.VMEM((model, kinds * DV), bf16),
            pltpu.VMEM((line * block, kinds * DV), bf16),
            pltpu.VMEM((line * block, 2 * DV), bf16),
            pltpu.VMEM((count, rows, 2 * DV), bf16),
            pltpu.VMEM((count, 2 * DV, out_weight.shape[1]), bf16),
            pltpu.VMEM((DR, DR), jnp.float32),
            pltpu.VMEM((rows, out_weight.shape[1]), jnp.float32),
            dma((5,)),
            dma,
            dma,
            dma((kinds + kinds // 2,)),
            dma((events,)),
            dma((events, parts)),
            dma((events,)),
            dma((events, parts)),
            dma,
            dma((count,)),
        ],
        compiler_params=pltpu.CompilerParams(
            collective_id=0, has_side_effects=True, vmem_limit_bytes=40000 * 1024
        ),
    )(
        *(pltpu.with_memory_space_constraint(a, pltpu.HBM) for a in operands)
    )


def body(tokens, norm_gain, *rest):
    weights, (map_lambda, diff_gain, decay_rate, state_gain, out_weight) = rest[:6], rest[6:]
    line = lax.axis_size("sp")
    pair = lax.axis_size("tp")
    local = map_lambda.shape[0]
    if local != line or line < 4 or decay_rate.shape[0] != local or lax.axis_size("fs") != 4 or pair != 2:
        return spread_body(tokens, norm_gain, *rest)
    return whole_layer(
        tokens[0],
        norm_gain,
        weights,
        map_lambda,
        diff_gain,
        decay_rate,
        state_gain,
        out_weight,
        line,
        pair,
    )[None]


def solution(mesh):
    placed = (
        P("fs", "sp", "tp"),
        P(),
        P("fs", "tp"),
        P("fs", "tp"),
        P("fs", "tp"),
        P("fs", "tp"),
        P("fs", "tp"),
        P("fs", "tp"),
        P("tp"),
        P("tp"),
        P("tp"),
        P("tp"),
        P(),
    )
    return jax.shard_map(
        body, mesh=mesh, in_specs=placed, out_specs=P("fs", ("sp", "tp"), None), check_vma=False
    )
```

```python
import functools

import jax
import jax.numpy as jnp
from jax import lax
from jax.experimental import pallas as pl
from jax.experimental.pallas import tpu as pltpu
from jax.sharding import PartitionSpec as P

DK = 64
DV = 128
DR = 128


epsilon = 1e-05
branch_scale = 0.8
masked_score = -1e30


def from_behind(x, axis, by):
    size = lax.axis_size(axis)
    pairs = [(i, i + by) for i in range(size) if 0 <= i + by < size]
    return lax.ppermute(x, axis, pairs)


def entering(x, axis, join, neutral):
    place = lax.axis_index(axis)
    gathered = jax.tree.map(
        lambda a, kind: lax.all_gather(a.astype(kind), axis), x, (jnp.bfloat16, jnp.bfloat16)
    )
    state = jax.tree.map(lambda a, e: jnp.zeros_like(a) + jnp.asarray(e, a.dtype), x, neutral)

    def one(turn, state):
        return join(
            state,
            jax.tree.map(
                lambda a, own: lax.dynamic_index_in_dim(a, turn, 0, False).astype(own.dtype),
                gathered,
                x,
            ),
        )

    return lax.fori_loop(0, place, one, state)


def attend(att_query, att_keys, att_values, map_lambda, diff_gain):
    tok_rows = att_query.shape[0]
    head_count = map_lambda.shape[0]
    key_width = att_keys.shape[1]
    query_heads = att_query.reshape(tok_rows, head_count, 2, DK)
    sp_index = lax.axis_index("sp")
    query_place = sp_index * tok_rows + jnp.arange(tok_rows)
    score_scale = DK ** (-0.5)

    def absorb_block(running, inputs):
        key_block, key_place = inputs
        key_heads = key_block[:, :key_width].reshape(tok_rows, head_count, 2, DK)
        value_heads = key_block[:, key_width:].reshape(tok_rows, head_count, DV)
        scores = (
            jnp.einsum(
                "qhmd,khmd->mhqk", query_heads, key_heads, preferred_element_type=jnp.float32
            )
            * score_scale
        )
        causal = key_place[None, :] <= query_place[:, None]
        row_peak, totals, summed = running
        new_peak = jnp.maximum(row_peak, jnp.max(jnp.where(causal, scores, masked_score), axis=-1))
        weights = jnp.where(causal, jnp.exp(scores - new_peak[..., None]), 0.0)
        factor = jnp.exp(row_peak - new_peak)
        totals = totals * factor + jnp.sum(weights, axis=-1)
        summed = summed * factor[..., None] + jnp.einsum(
            "mhqk,khv->mhqv",
            weights.astype(jnp.bfloat16),
            value_heads,
            preferred_element_type=jnp.float32,
        )
        return ((new_peak, totals, summed), None)

    def absorb(running, pieces, first_row):
        piece_rows = pieces.shape[0]
        stacked = pieces.reshape(piece_rows // tok_rows, tok_rows, pieces.shape[1])
        places = (first_row + jnp.arange(piece_rows)).reshape(piece_rows // tok_rows, tok_rows)
        return lax.scan(absorb_block, running, (stacked, places))[0]

    starting = (
        jnp.full((2, head_count, tok_rows), masked_score, jnp.float32),
        jnp.zeros((2, head_count, tok_rows), jnp.float32),
        jnp.zeros((2, head_count, tok_rows, DV), jnp.float32),
    )
    joined_kv = jnp.concatenate([att_keys, att_values], axis=1)
    first_state = absorb(starting, joined_kv, sp_index * tok_rows)

    def relay_step(step_index, relay_state):
        running, moving = relay_state
        moving = from_behind(moving, "sp", 1)
        first_row = (sp_index - step_index) * tok_rows
        running = lax.cond(
            first_row >= 0,
            lambda holding: absorb(holding, moving, first_row),
            lambda holding: holding,
            running,
        )
        return (running, moving)

    running, _ = lax.fori_loop(1, lax.axis_size("sp"), relay_step, (first_state, joined_kv))
    row_peak, totals, summed = running
    averaged = summed / totals[..., None]
    differ = averaged[0] - map_lambda[:, None, None] * averaged[1]
    normed = differ * lax.rsqrt(jnp.mean(differ * differ, axis=-1, keepdims=True) + epsilon)
    normed = normed * diff_gain.reshape(head_count, 1, DV) * branch_scale
    return normed.transpose(1, 0, 2).reshape(tok_rows, head_count * DV).astype(jnp.bfloat16)


def retain(ret_query, ret_keys, ret_values, decay_rate, state_gain):
    tok_rows = ret_query.shape[0]
    head_count = decay_rate.shape[0]
    query_heads = ret_query.reshape(tok_rows, head_count, DR)
    key_heads = ret_keys.reshape(tok_rows, head_count, DR)
    value_heads = ret_values.reshape(tok_rows, head_count, DR)
    position = jnp.arange(tok_rows).astype(jnp.float32)
    distance = position[:, None] - position[None, :]
    decay_col = decay_rate[:, None, None]
    within = jnp.where(distance >= 0, jnp.exp(-decay_col * jnp.maximum(distance, 0.0)), 0.0)
    local_scores = (
        jnp.einsum("qhd,khd->hqk", query_heads, key_heads, preferred_element_type=jnp.float32)
        * within
    )
    intra_out = jnp.einsum(
        "hqk,khv->hqv",
        local_scores.astype(jnp.bfloat16),
        value_heads,
        preferred_element_type=jnp.float32,
    )
    key_decayed = key_heads.astype(jnp.float32) * jnp.exp(
        -decay_rate[None, :, None] * (tok_rows - 1.0 - position)[:, None, None]
    )
    own_state = jnp.einsum(
        "khd,khv->hdv",
        key_decayed,
        value_heads.astype(jnp.float32),
        precision=lax.Precision.HIGHEST,
    )
    block_decay = jnp.exp(-decay_rate * tok_rows)

    def link_states(earlier, later):
        return (earlier[0] * later[1][:, None, None] + later[0], earlier[1] * later[1])

    identity = (jnp.zeros_like(own_state), jnp.ones_like(block_decay))
    incoming, _ = entering((own_state, block_decay), "sp", link_states, identity)
    carried = jnp.einsum(
        "qhd,hdv->hqv", query_heads.astype(jnp.float32), incoming, precision=lax.Precision.HIGHEST
    )
    carried = carried * jnp.exp(-decay_col * (position + 1.0)[None, :, None])
    combined = intra_out + carried
    normed = combined * lax.rsqrt(jnp.mean(combined * combined, axis=-1, keepdims=True) + epsilon)
    normed = normed * state_gain.reshape(head_count, 1, DR)
    return normed.transpose(1, 0, 2).reshape(tok_rows, head_count * DR).astype(jnp.bfloat16)


def spread_body(
    tokens,
    norm_gain,
    query_weight,
    key_weight,
    value_weight,
    state_query,
    state_key,
    state_value,
    map_lambda,
    diff_gain,
    decay_rate,
    state_gain,
    out_weight,
):
    gathered = lax.all_gather(tokens[0], "tp", axis=1, tiled=True)
    tok_float = gathered.astype(jnp.float32)
    normed = tok_float * lax.rsqrt(
        jnp.mean(tok_float * tok_float, axis=-1, keepdims=True) + epsilon
    )
    normed = (normed * norm_gain).astype(jnp.bfloat16)
    pieces = (
        lax.all_gather(query_weight, "fs", axis=0, tiled=True),
        lax.all_gather(key_weight, "fs", axis=0, tiled=True),
        lax.all_gather(value_weight, "fs", axis=0, tiled=True),
        lax.all_gather(state_query, "fs", axis=0, tiled=True),
        lax.all_gather(state_key, "fs", axis=0, tiled=True),
        lax.all_gather(state_value, "fs", axis=0, tiled=True),
    )
    projected = tuple(
        (jnp.dot(normed, row_block, preferred_element_type=jnp.float32) for row_block in pieces)
    )
    att_query, att_keys, att_values, ret_query, ret_keys, ret_values = (
        member.astype(jnp.bfloat16) for member in projected
    )
    attended = attend(att_query, att_keys, att_values, map_lambda, diff_gain)
    retained = retain(ret_query, ret_keys, ret_values, decay_rate, state_gain)
    joined = jnp.concatenate([attended, retained], axis=1)
    diff_width = attended.shape[1]
    ret_width = retained.shape[1]
    tp_count = lax.axis_size("tp")
    tp_index = lax.axis_index("tp")
    own_rows = jnp.concatenate(
        [
            lax.dynamic_slice_in_dim(out_weight, tp_index * diff_width, diff_width, 0),
            lax.dynamic_slice_in_dim(
                out_weight, tp_count * diff_width + tp_index * ret_width, ret_width, 0
            ),
        ],
        axis=0,
    )
    output = lax.psum_scatter(
        jnp.dot(joined, own_rows, preferred_element_type=jnp.float32).astype(jnp.bfloat16),
        "tp",
        scatter_dimension=0,
        tiled=True,
    )
    return output[None]


def row_product(a, b):
    return lax.dot_general(a, b, (((1,), (1,)), ((), ())), preferred_element_type=jnp.float32)


MESH = pl.DeviceIdType.MESH


def greet(peers):
    barrier = pltpu.get_barrier_semaphore()
    count = 0
    for peer, present in peers:
        if present is None:
            pl.semaphore_signal(barrier, inc=1, device_id=peer, device_id_type=MESH)
            count = count + 1
        else:

            @pl.when(present)
            def _():
                pl.semaphore_signal(barrier, inc=1, device_id=peer, device_id_type=MESH)

            count = count + jnp.where(present, 1, 0)
    pl.semaphore_wait(barrier, count)


def layer_kernel(
    line,
    parts,
    tokens,
    gain_in,
    w0,
    w1,
    w2,
    w3,
    w4,
    w5,
    lam_in,
    dgain_in,
    rate_in,
    sgain_in,
    out_weight,
    result,
    gains,
    lam_ref,
    rate_ref,
    seq,
    normal,
    weight,
    proj,
    mine,
    joined,
    held,
    state,
    total,
    local_sem,
    held_sem,
    wsend,
    wrecv,
    lsend,
    lrecv,
    psend,
    precv,
    osend,
    orecv,
):
    f32, bf16 = jnp.float32, jnp.bfloat16
    weights = (w0, w1, w2, w3, w4, w5)
    kinds = len(weights)
    half_kinds = kinds // 2
    early_parts = parts // 2
    events = 2 * line - 1
    z, f, c = lax.axis_index("sp"), lax.axis_index("fs"), lax.axis_index("tp")
    block, half = tokens.shape
    piece = block // parts
    depth = w0.shape[0]
    width = weight.shape[1] // kinds
    rows_out = result.shape[0]
    model = seq.shape[1]
    me = c * line + z
    near = ({"fs": f ^ 1}, {"fs": f ^ 2})
    whose = (f ^ 1, f ^ 2, f ^ 3)
    def held_at(b, side, q):
        return seq.at[
            pl.ds(pl.multiple_of(b * block + q * piece, piece), piece),
            pl.ds(pl.multiple_of(side * half, half), half),
        ]

    def whole(b, side):
        return seq.at[
            pl.ds(pl.multiple_of(b * block, block), block),
            pl.ds(pl.multiple_of(side * half, half), half),
        ]

    def column(kind):
        return (2 * (kind % half_kinds) + kind // half_kinds) * width

    def stored(owner, kind):
        return weight.at[
            pl.ds(pl.multiple_of(owner * depth, depth), depth), column(kind) : column(kind) + width
        ]

    def slot(e):
        up = (e - 1) % 2 == 0
        s = (e - 1) // 2
        return z - 1 - s if up else z + 1 + s

    def along(e, b, q):
        target = z + 1 if (e - 1) % 2 == 0 else z - 1
        return pltpu.make_async_remote_copy(
            src_ref=held_at(b, c, q),
            dst_ref=held_at(b, c, q),
            send_sem=lsend.at[e],
            recv_sem=lrecv.at[e, q],
            device_id={"sp": jnp.clip(target, 0, line - 1)},
            device_id_type=MESH,
        ), (target >= 0) & (target < line)

    def across(e, b, side, q):
        return pltpu.make_async_remote_copy(
            src_ref=held_at(b, side, q),
            dst_ref=held_at(b, side, q),
            send_sem=psend,
            recv_sem=precv.at[e, q],
            device_id={"tp": 1 - c},
            device_id_type=MESH,
        )

    def all_along(e):
        return pltpu.make_async_remote_copy(
            src_ref=whole(z, c),
            dst_ref=whole(z, c),
            send_sem=lsend.at[e],
            recv_sem=lrecv.at[e, 0],
            device_id={"sp": z ^ 1},
            device_id_type=MESH,
        )

    def all_across():
        columns = seq.at[:, pl.ds(pl.multiple_of(c * half, half), half)]
        return pltpu.make_async_remote_copy(
            src_ref=columns,
            dst_ref=columns,
            send_sem=psend,
            recv_sem=precv.at[0, 0],
            device_id={"tp": 1 - c},
            device_id_type=MESH,
        )

    def own_columns(kind):
        return weights[kind].at[:, pl.ds(pl.multiple_of(z * width, width), width)]

    def arrival(relation, kind):
        return kind if relation == kind // half_kinds else kinds + kind % half_kinds

    def spread(way, kind, source, owner, index):
        return pltpu.make_async_remote_copy(
            src_ref=source,
            dst_ref=stored(owner, kind),
            send_sem=wsend,
            recv_sem=wrecv.at[arrival(2 if index >= kinds else way, kind)],
            device_id=near[way],
            device_id_type=MESH,
        )

    def arrived(relation, kind):
        pltpu.make_async_remote_copy(
            src_ref=stored(whose[relation], kind),
            dst_ref=stored(whose[relation], kind),
            send_sem=wsend,
            recv_sem=wrecv.at[arrival(relation, kind)],
            device_id=near[0],
            device_id_type=MESH,
        ).wait_recv()

    def push(e, q, when=True):
        copy, present = along(e, z, q)

        @pl.when(present & when)
        def _():
            copy.start()

    def scatter(pair):
        for turn in range(2):
            for way in range(2):
                kind = pair + half_kinds * (turn ^ way)
                spread(way, kind, stored(f, kind), f, kind).start()

    first_copies = [pltpu.make_async_copy(tokens, whole(z, c), local_sem.at[0])]
    for kind in range(kinds):
        first_copies.append(
            pltpu.make_async_copy(own_columns(kind), stored(f, kind), local_sem.at[1])
        )
    for copy in first_copies:
        copy.start()
    greet(
        [
            (near[0], None),
            (near[1], None),
            ({"tp": 1 - c}, None),
            ({"sp": jnp.minimum(z + 1, line - 1)}, z + 1 < line),
            ({"sp": jnp.maximum(z - 1, 0)}, z > 0),
        ]
    )
    first_copies[0].wait()
    for q in range(parts):
        push(1, q, z >= 0 if q < early_parts else z == 0)
        push(2, q)
    own_rows = weight.at[pl.ds(pl.multiple_of(f * depth, depth), depth), :]
    pltpu.make_async_copy(own_rows, own_rows, local_sem.at[1]).wait()
    scatter(0)
    for q in range(parts):
        across(0, z, c, q).start()
    scatter(1)
    spots = ((gain_in, 0), (dgain_in, model), (sgain_in, model + dgain_in.shape[1]))
    for source, first in spots:
        pltpu.make_async_copy(
            source, gains.at[:, first : first + source.shape[1]], local_sem.at[2]
        ).start()
    rates = (
        pltpu.make_async_copy(lam_in, lam_ref, local_sem.at[3]),
        pltpu.make_async_copy(rate_in, rate_ref, local_sem.at[4]),
    )
    for copy in rates:
        copy.start()

    def relay(turn):
        for way in range(2):
            kind = turn + way * half_kinds
            arrived(way, kind)
            spread(1 - way, kind, stored(whose[way], kind), whose[way], kinds + turn).start()

    def complete(turn):
        landed = weight.at[: 2 * depth, 2 * turn * width : 2 * (turn + 1) * width]
        pltpu.make_async_remote_copy(
            src_ref=landed,
            dst_ref=landed,
            send_sem=wsend,
            recv_sem=wrecv.at[kinds + turn],
            device_id=near[0],
            device_id_type=MESH,
        ).wait_recv()

    def serve(e, q, when):
        b = slot(e)

        @pl.when((b >= 0) & (b < line) & when)
        def _():
            copy, _ = along(e, b, q)
            copy.wait_recv()
            if (e - 1) // 2 + 1 < line - 1:
                onward, present = along(e + 2, b, q)

                @pl.when(present)
                def _():
                    onward.start()

            across(e, b, c, q).start()

    def at_slot(k):
        for s in range(line - 1):
            for q in range(parts):
                if q < early_parts:
                    if k == s * early_parts + q:
                        serve(1 + 2 * s, q, z > s)
                else:
                    for other in range(s + 1, line):
                        if k == (2 * other - 4 - s) * early_parts + parts + q:
                            serve(1 + 2 * s, q, z == other)
        serve(2 + 2 * (k // parts), k % parts, z >= 0)
        if k % parts == parts - 1 and k // parts < line - 2:
            for q in range(early_parts, parts):
                push(1, q, z == k // parts + 1)

    def fetch(index):
        source = index // 2
        kind = index % 2
        first = kind * (out_weight.shape[0] // 2) + source * width
        return pltpu.make_async_copy(
            out_weight.at[first : first + width, :],
            held.at[source, kind * width : (kind + 1) * width, :],
            held_sem,
        )

    fetches = [fetch(index) for index in range(2 * joined.shape[0])]

    def block_of(e):
        s = (e - 1) // 2
        return jnp.where(e == 0, z, jnp.where((e - 1) % 2 == 0, z - 1 - s, z + 1 + s))

    def rows_of(b):
        return pl.ds(pl.multiple_of(b * block, block), block)

    def normalize(e, b):
        for q in range(parts):
            across(e, b, 1 - c, q).wait_recv()
        x = seq[rows_of(b), :].astype(f32)
        scaled = x * lax.rsqrt(jnp.mean(x * x, axis=1, keepdims=True) + epsilon)
        normal[rows_of(b), :] = (scaled * gains[:, :model]).astype(bf16)

    def project(b, first, count):
        columns = slice(2 * first * width, 2 * (first + count) * width)
        proj[rows_of(b), columns] = jnp.dot(
            normal[rows_of(b), :], weight[:, columns], preferred_element_type=f32
        ).astype(bf16)

    def soon(e, b):
        return (e == 0) | (((e == 2) | ((e == 1) & (z == 1))) & (b < line))

    def late(e):
        return ((z == line - 1) & (e % 2 == 1) & (e < events - 2)) | ((z == 0) & (e == events - 1))

    def normalize_some(first, last, chosen):
        def one(e, carry):
            b = block_of(e)

            @pl.when((b >= 0) & (b < line) & chosen(e, b))
            def _():
                normalize(e, b)

            return carry

        lax.fori_loop(first, last, one, 0)

    def project_ready(first, count):
        def one(b, carry):
            @pl.when(
                ((z > 0) | (b < line - 1)) & ((z < line - 1) | (b == 0) | (b == line - 1))
            )
            def _():
                project(b, first, count)

            return carry

        lax.fori_loop(0, line, one, 0)

    early_slots = parts * (line - 2)
    relay(0)
    scatter(2)
    for copy in fetches:
        copy.start()
    for k in range(early_slots):
        at_slot(k)
        if k < 2:
            relay(k + 1)
        if k == parts:
            for copy in rates:
                copy.wait()
            pltpu.make_async_copy(gains, gains, local_sem.at[2]).wait()
            normalize_some(0, 3, soon)
    normalize_some(1, events, lambda e, b: ~soon(e, b) & ~late(e))
    for turn in range(half_kinds - 1):
        complete(turn)
    project_ready(0, half_kinds - 1)
    complete(half_kinds - 1)
    project_ready(half_kinds - 1, 1)

    row = lax.broadcasted_iota(jnp.int32, (block, block), 0)
    col = lax.broadcasted_iota(jnp.int32, (block, block), 1)
    lane = lax.broadcasted_iota(jnp.int32, (block, 2 * DK), 1)
    position = lax.broadcasted_iota(jnp.int32, (block, 1), 0).astype(f32)

    def part(kind, first, count):
        return proj[first : first + count, column(kind) : column(kind) + DV]

    def mix(b):
        first = b * block
        causal = col <= row
        lam = lam_ref[z]
        rate = rate_ref[z]
        query = part(0, first, block) * jnp.asarray(DK ** (-0.5), bf16)
        averaged = []
        for which in range(2):
            own = jnp.where((lane >= DK) == bool(which), query, jnp.zeros_like(query))
            near_scores = jnp.where(causal, row_product(own, part(1, first, block)), masked_score)
            peak = jnp.max(near_scores, axis=1, keepdims=True)
            if first:
                far = row_product(own, part(1, 0, first))
                peak = jnp.maximum(peak, jnp.max(far, axis=1, keepdims=True))
            near_scores = jnp.exp(near_scores - peak)
            count = jnp.sum(near_scores, axis=1, keepdims=True)
            summed = jnp.dot(
                near_scores.astype(bf16), part(2, first, block), preferred_element_type=f32
            )
            if first:
                far = jnp.exp(far - peak)
                count = count + jnp.sum(far, axis=1, keepdims=True)
                summed = summed + jnp.dot(
                    far.astype(bf16), part(2, 0, first), preferred_element_type=f32
                )
            averaged.append(summed / count)
        differ = averaged[0] - lam * averaged[1]
        scaled = differ * lax.rsqrt(jnp.mean(differ * differ, axis=1, keepdims=True) + epsilon)
        mine[first : first + block, :DV] = (
            scaled * (gains[:, pl.ds(pl.multiple_of(model + z * DV, DV), DV)] * branch_scale)
        ).astype(bf16)
        ret_query = part(3, first, block)
        ret_keys = part(4, first, block)
        ret_values = part(5, first, block)
        within = jnp.where(causal, jnp.exp(-rate * jnp.maximum(row - col, 0).astype(f32)), 0.0)
        local = (row_product(ret_query, ret_keys) * within).astype(bf16)
        mixed = jnp.dot(local, ret_values, preferred_element_type=f32)
        if first:
            mixed = mixed + jnp.exp(-rate * (position + 1.0)) * jnp.dot(
                ret_query, state[...].astype(bf16), preferred_element_type=f32
            )
        if b + 1 < line:
            decayed = (ret_keys.astype(f32) * jnp.exp(-rate * (block - 1.0 - position))).astype(bf16)
            update = lax.dot_general(
                decayed, ret_values, (((0,), (0,)), ((), ())), preferred_element_type=f32
            )
            if first:
                update = state[...] * jnp.exp(jnp.full((1, DR), -block, f32) * rate) + update
            state[...] = update
        scaled = mixed * lax.rsqrt(jnp.mean(mixed * mixed, axis=1, keepdims=True) + epsilon)
        mine[first : first + block, DV:] = (scaled * gains[:, pl.ds(pl.multiple_of(model + dgain_in.shape[1] + z * DV, DV), DV)]).astype(bf16)

    def mine_rows(b, side):
        return mine.at[pl.ds(pl.multiple_of(b * block + side * rows_out, rows_out), rows_out), :]

    def deliver(b, h):
        return pltpu.make_async_remote_copy(
            src_ref=mine_rows(b, h),
            dst_ref=joined.at[me],
            send_sem=osend,
            recv_sem=orecv.at[me],
            device_id={"sp": b, "tp": h},
            device_id_type=MESH,
        )

    def own_place(b, h):
        return (z == b) & (c == h)

    def send(b, when, halves=(0, 1)):
        for h in halves:

            @pl.when(when & ~own_place(b, h))
            def _():
                deliver(b, h).start()

    def give(b):
        if b == 0:
            send(b, z <= 1)
        elif b == line - 1:
            send(b, (z == 0) | (z >= line - 2))
        else:
            send(b, z >= 0)

        @pl.when(z == b)
        def _():
            joined[me] = mine_rows(b, c)[...]

    def phase(t, carry):
        @pl.when(t == line - 2)
        def _():
            send(0, (z > 1) & (z < line - 1))
            send(0, z == line - 1, (1,))
            send(line - 1, (z > 0) & (z < line - 2))

        @pl.when(t == line - 3)
        def _():
            send(0, z == line - 1, (0,))

        for turn in range(1, line - 1):

            @pl.when(t == turn)
            def _():
                for q in range(early_parts):
                    at_slot(early_slots + (turn - 1) * early_parts + q)

        @pl.when((t > 0) & ((z == line - 1) | ((z == 0) & (t <= parts))))
        def _():
            b = jnp.where(z == 0, line - 1, t)
            e = jnp.where(z == 0, events - 1, 2 * (line - 2 - t) + 1)

            def one(q, carry):
                across(e, b, 1 - c, q).wait_recv()
                rows = pl.ds(pl.multiple_of(b * block + q * piece, piece), piece)
                x = seq[rows, :].astype(f32)
                scaled = x * lax.rsqrt(jnp.mean(x * x, axis=1, keepdims=True) + epsilon)
                normal[rows, :] = (scaled * gains[:, :model]).astype(bf16)
                proj[rows, :] = jnp.dot(
                    normal[rows, :], weight[...], preferred_element_type=f32
                ).astype(bf16)
                return carry

            lax.fori_loop(
                jnp.where(z == 0, t - 1, 0), jnp.where(z == 0, t, parts), one, 0
            )

        for b in range(line):
            turn = jnp.where(z == line - 1, min(b, line - 2), 0)
            if b == line - 1:
                turn = jnp.where(z == 0, line - 2, turn)

            @pl.when(turn == t)
            def _():
                mix(b)
                give(b)

        return carry

    lax.fori_loop(0, line - 1, phase, 0)

    sent = weight.at[: 3 * depth, :]
    pltpu.make_async_remote_copy(
        src_ref=sent,
        dst_ref=sent,
        send_sem=wsend,
        recv_sem=wrecv.at[0],
        device_id=near[0],
        device_id_type=MESH,
    ).wait_send()
    all_across().wait_send()
    for e in range(1, events):
        up = e % 2 == 1
        target = z + 1 if up else z - 1
        s = (e - 1) // 2
        source = z - s if up else z + s
        present = (target >= 0) & (target < line) & (source >= 0) & (source < line)

        @pl.when(present)
        def _():
            all_along(e).wait_send()

    pltpu.make_async_copy(held, held, held_sem).wait()
    inner = [s for s in range(1, line - 1)]
    outer = (z == 0) | (z == line - 1)
    order = []
    for index in range(line):
        for_outer = ([0, line - 1] + inner)[index]
        for_inner = (inner + [0, line - 1])[index]
        order.append(jnp.where(outer, for_outer, for_inner))
    for index, source in enumerate(order):
        for turn in range(2):
            side = c if turn == 0 else 1 - c
            where = side * line + source

            @pl.when(where != me)
            def _():
                pltpu.make_async_remote_copy(
                    src_ref=joined.at[where],
                    dst_ref=joined.at[where],
                    send_sem=osend,
                    recv_sem=orecv.at[where],
                    device_id={"tp": 1 - c},
                    device_id_type=MESH,
                ).wait_recv()

            product = jnp.dot(joined[where], held[where], preferred_element_type=f32)
            if index == 0 and turn == 0:
                total[...] = product
            elif index < line - 1 or turn == 0:
                total[...] += product
            else:
                result[...] = (total[...] + product).astype(bf16)

    gone = mine.at[: (2 * line - 1) * rows_out, :]
    pltpu.make_async_remote_copy(
        src_ref=gone,
        dst_ref=gone,
        send_sem=osend,
        recv_sem=orecv.at[0],
        device_id={"tp": 1 - c},
        device_id_type=MESH,
    ).wait_send()


def whole_layer(tokens, norm_gain, weights, map_lambda, diff_gain, decay_rate, state_gain, out_weight, line, pair):
    block, half = tokens.shape
    kinds = len(weights)
    model = norm_gain.shape[0]
    parts = 2
    rows = block // pair
    count = line * pair
    anywhere = pl.BlockSpec(memory_space=pl.ANY)
    vmem = pl.BlockSpec(memory_space=pltpu.VMEM)
    events = 2 * line - 1
    dma = pltpu.SemaphoreType.DMA
    bf16 = jnp.bfloat16
    operands = (
        tokens,
        norm_gain[None],
        *weights,
        map_lambda,
        diff_gain[None],
        decay_rate,
        state_gain[None],
        out_weight,
    )
    return pl.pallas_call(
        functools.partial(layer_kernel, line, parts),
        out_shape=jax.ShapeDtypeStruct((rows, out_weight.shape[1]), bf16),
        in_specs=[anywhere] * (kinds + 7),
        out_specs=vmem,
        scratch_shapes=[
            pltpu.VMEM((1, model + diff_gain.shape[0] + state_gain.shape[0]), jnp.float32),
            pltpu.SMEM(map_lambda.shape, jnp.float32),
            pltpu.SMEM(decay_rate.shape, jnp.float32),
            pltpu.VMEM((line * block, model), bf16),
            pltpu.VMEM((line * block, model), bf16),
            pltpu.VMEM((model, kinds * DV), bf16),
            pltpu.VMEM((line * block, kinds * DV), bf16),
            pltpu.VMEM((line * block, 2 * DV), bf16),
            pltpu.VMEM((count, rows, 2 * DV), bf16),
            pltpu.VMEM((count, 2 * DV, out_weight.shape[1]), bf16),
            pltpu.VMEM((DR, DR), jnp.float32),
            pltpu.VMEM((rows, out_weight.shape[1]), jnp.float32),
            dma((5,)),
            dma,
            dma,
            dma((kinds + kinds // 2,)),
            dma((events,)),
            dma((events, parts)),
            dma,
            dma((events, parts)),
            dma,
            dma((count,)),
        ],
        compiler_params=pltpu.CompilerParams(
            collective_id=0, has_side_effects=True, vmem_limit_bytes=40000 * 1024
        ),
    )(
        *(pltpu.with_memory_space_constraint(a, pltpu.HBM) for a in operands)
    )


def body(tokens, norm_gain, *rest):
    weights, (map_lambda, diff_gain, decay_rate, state_gain, out_weight) = rest[:6], rest[6:]
    line = lax.axis_size("sp")
    pair = lax.axis_size("tp")
    local = map_lambda.shape[0]
    if local != line or line < 4 or decay_rate.shape[0] != local or lax.axis_size("fs") != 4 or pair != 2:
        return spread_body(tokens, norm_gain, *rest)
    return whole_layer(
        tokens[0],
        norm_gain,
        weights,
        map_lambda,
        diff_gain,
        decay_rate,
        state_gain,
        out_weight,
        line,
        pair,
    )[None]


def solution(mesh):
    placed = (
        P("fs", "sp", "tp"),
        P(),
        P("fs", "tp"),
        P("fs", "tp"),
        P("fs", "tp"),
        P("fs", "tp"),
        P("fs", "tp"),
        P("fs", "tp"),
        P("tp"),
        P("tp"),
        P("tp"),
        P("tp"),
        P(),
    )
    return jax.shard_map(
        body, mesh=mesh, in_specs=placed, out_specs=P("fs", ("sp", "tp"), None), check_vma=False
    )
```
